32 devices in a mesh: sp: 4 (over z), tp: 8 (over y, x, core).
Axes of the slice: x: 2, y: 2, z: 4, core: 2. Of those that a mesh axis runs over, the one named last changes fastest.
Arguments:
- token_values: bfloat16 [1024, 2048], P('sp', 'tp'), may hold values from -6 to 6
- write_keys: bfloat16 [1024, 1024], P('sp', 'tp'), may hold values from -0.4375 to 0.4375
- read_keys: bfloat16 [1024, 1024], P('sp', 'tp'), may hold values from -0.4375 to 0.4375
- log_decay: float32 [32, 1024], P('tp', 'sp'), may hold values from -0.7 to 0, as said below
- out_gate: bfloat16 [1024, 2048], P('sp', 'tp'), may hold values from -6 to 6
- out_proj: bfloat16 [4096, 2048], P(None, 'tp'), may hold values from -0.125 to 0.125
- mixed: bfloat16 [1024, 4096], P('sp'), may hold values from -6 to 6
- cotangent: bfloat16 [1024, 4096], P('sp'), may hold values from -8 to 8
- route_ids: int32 [1024, 2], P('sp'), may hold values from 0 to 3, all different within a row; in each aligned block of 256 rows (0 to 255, 256 to 511, ...) at most 192 rows name the same one
- route_weights: float32 [1024, 2], P('sp'), may hold values from 0.25 to 1
- w_gate: bfloat16 [4, 4096, 2048], P('sp', None, 'tp'), may hold values from -0.09375 to 0.09375
- w_up: bfloat16 [4, 4096, 2048], P('sp', None, 'tp'), may hold values from -0.09375 to 0.09375
- w_down: bfloat16 [4, 2048, 4096], P('sp', 'tp'), may hold values from -0.125 to 0.125
Outputs:
- value_grad: bfloat16 [1024, 2048], P('sp', 'tp')
- write_grad: bfloat16 [1024, 1024], P('sp', 'tp')
- read_grad: bfloat16 [1024, 1024], P('sp', 'tp')
- gate_grad: bfloat16 [1024, 2048], P('sp', 'tp')
- proj_grad: float32 [4096, 2048], P('sp', 'tp')
- gate_weight_grad: bfloat16 [4, 4096, 2048], P('sp', None, 'tp')
- up_weight_grad: bfloat16 [4, 4096, 2048], P('sp', None, 'tp')
- down_weight_grad: bfloat16 [4, 2048, 4096], P('sp', 'tp')
The draws below stay inside these ranges and needn't reach their ends.
Inputs may be any that keep to these rules, and one draw needn't show every extreme that they name: `route_ids`: each row names 2 different experts. Within the rows of one device no expert is named more than 192 times, and in every draw some expert is named exactly 192 times by the rows of some device. `log_decay`: every entry is negative.
All inputs are finite; a program needn't handle non-finite values.
Results may differ from the reference program's by a relative error of at most 0.019.
Values may be sent and summed in bfloat16 or wider, within the bound.
A program may use at most 128 MiB of HBM per device.

```python
import math
import jax
import jax.numpy as jnp
import numpy as np
from jax import lax

D = 4096
GROUPS = 8
HEAD_DIM = 64
STATE = 128
HEADS = 32
INNER = 2048
EXPERT_HIDDEN_SIZE = 2048
TOP = 2
BLOCK = 64
TOK_DEV = 256
TOKENS = 1024
EXPERTS = 4
CAP = 192
N_SP = 4
N_TP = 8


def draw_log_decay(key, part):
    keys = jax.random.split(jax.random.fold_in(key, 7), 7)
    fast_share = 0.5
    fast = jax.random.uniform(keys[0], (HEADS, 1), jnp.float32) < fast_share
    fast_rate = jnp.exp(jax.random.uniform(keys[1], (HEADS, 1), jnp.float32, jnp.log(2.3 / 50.0), jnp.log(2.3 / 30.0)))
    keep = jax.random.uniform(keys[2], (HEADS, 1), jnp.float32, 0.55, 0.8)
    slow_rate = -jnp.log(keep) / TOKENS
    segment_factor = jnp.exp(jax.random.uniform(keys[3], (HEADS, TOKENS // TOK_DEV), jnp.float32, -0.45, 0.45))
    segment_factor = jnp.repeat(segment_factor, TOK_DEV, axis=1)
    token_factor = jnp.exp(jax.random.uniform(keys[4], (HEADS, TOKENS), jnp.float32, -0.6, 0.6))
    decay_speed = jnp.where(fast, fast_rate, slow_rate) * segment_factor * token_factor
    positions = jax.random.randint(keys[5], (HEADS, 2), 0, TOKENS)
    gate_intensity = jax.random.uniform(keys[6], (HEADS, 2), jnp.float32, jnp.log(0.5), jnp.log(0.8))
    places = jnp.arange(TOKENS, dtype=jnp.int32)
    dropped_tokens = places[None, None, :] == positions[:, :, None]
    decay_pulse = jnp.sum(jnp.where(dropped_tokens, gate_intensity[:, :, None], 0.0), axis=1)
    return jnp.clip(decay_pulse - decay_speed, -0.7, -1e-06).astype(jnp.float32)


def strengthened(drawn, stream_key, source, target, shards_of, factor):
    def block_of(dim):
        return (jnp.arange(drawn.shape[dim]) // (drawn.shape[dim] // shards_of)).reshape((-1,) + (1,) * (drawn.ndim - 1 - dim))

    first = jax.random.permutation(stream_key, shards_of)[block_of(target)]
    second = (block_of(target) + shards_of // 2) % shards_of
    return jnp.where((block_of(source) == first) | (block_of(source) == second), factor * drawn, drawn)


def shard_levels(own_key, dims, cuts, smallest, high):
    loudness, own = 1.0, jax.random.fold_in(own_key, 6)
    for dim, parts in cuts:
        heights = jnp.exp(jax.random.uniform(jax.random.fold_in(own, dim), (parts,), jnp.float32, smallest / len(cuts), high / len(cuts)))
        loudness = loudness * jnp.repeat(heights, dims[dim] // parts).reshape([-1 if axis == dim else 1 for axis in range(len(dims))])
    return loudness


def deal_out(stream_key, own, number, rows, number_of, top, bound, skew):
    order = jax.random.permutation(stream_key, number_of)
    crowded, usual = shares(number_of, rows * top, bound, skew, True), shares(number_of, rows * top, bound, skew, False)
    places = jnp.arange(number_of)

    def named(sizes, rotation):
        used = int((sizes > 0).sum())
        fixed = max(1, used // 4)
        passed = fixed + (places - fixed + rotation * (used - fixed)) % max(1, number_of - fixed)
        return jnp.zeros((number_of,), jnp.int32).at[order[jnp.where(places < fixed, places, passed)]].set(jnp.asarray(sizes, jnp.int32))

    sizes = jnp.where(number % 4 == 0, named(crowded, number // 4), named(usual, number - number // 4 - 1))
    mixed = jax.random.permutation(jax.random.fold_in(own, 3), number_of)
    source_of, receiver = mixed[0:number_of // 2 * 2:2], mixed[1:number_of // 2 * 2:2]
    margin = jnp.minimum(sizes[source_of] - 1, bound - sizes[receiver]) // 2
    margin = jnp.where((source_of == order[0]) | (receiver == order[0]) | (sizes[receiver] == 0), 0, jnp.maximum(margin, 0))
    passed = jax.random.randint(jax.random.fold_in(own, 4), (number_of // 2,), 0, 1 << 20) % (margin + 1)
    sizes = sizes.at[source_of].add(-passed).at[receiver].add(passed)
    items = jnp.searchsorted(jnp.cumsum(sizes), jnp.arange(rows * top), side="right").astype(jnp.int32)
    table = items.reshape(top, rows).T
    table = table[jax.random.permutation(jax.random.fold_in(own, 1), rows)]
    rotation = jax.random.randint(jax.random.fold_in(own, 2), (rows, 1), 0, top)
    return jnp.take_along_axis(table, (jnp.arange(top)[None, :] + rotation) % top, axis=1)


def shares(count, total, reach, lean, full):
    portions = [(1 << 20) // math.isqrt(rank ** lean) + 1 for rank in range(1, count + 1)]
    largest = reach if full else min(reach, max(-(-total // count), total * portions[0] // sum(portions)))
    least = 1 if total - largest >= count - 1 else 0
    holding, rest = [largest] + [least] * (count - 1), total - largest - least * (count - 1)
    while rest > 0:
        candidates = [i for i in range(1, count) if holding[i] < largest] or [i for i in range(1, count) if holding[i] < reach]
        whole, budget = sum([portions[i] for i in candidates]), rest
        for i in candidates:
            more = min(reach - holding[i], max(1, budget * portions[i] // whole), rest)
            holding[i] = holding[i] + more
            rest = rest - more
    return np.array(holding)


def centred(key, extent, scale, most, cuts=(), held_as=jnp.bfloat16):
    level = shard_levels(key, extent, cuts, -0.22, 0.18) if cuts else 1.0
    array = jax.random.normal(key, extent, jnp.float32) * scale * level
    return jnp.minimum(jnp.maximum(array, -most), most).astype(held_as)


def gaussian_with(stream_key, shape, deviation, most, shards, heavy, held_as=jnp.bfloat16):
    result = deviation * jax.random.normal(stream_key, shape, jnp.float32)
    if shards:
        result = result * shard_levels(stream_key, shape, shards, -0.22, 0.18)
    return jnp.clip(strengthened(result, jax.random.fold_in(stream_key, 3), *heavy), -most, most).astype(held_as)


def setup_inputs(seed: int = 0) -> dict:
    splits = jax.random.split(jax.random.key(seed), 14)
    token_values = centred(splits[0], (TOKENS, INNER), 1.0, 6.0, ((0, 4), (1, 8)))
    write_keys = centred(splits[1], (TOKENS, GROUPS * STATE), ((TOKENS * STATE // 4) ** -0.25), 0.4375, ((0, 4), (1, 8)))
    read_keys = centred(splits[2], (TOKENS, GROUPS * STATE), ((TOKENS * STATE // 4) ** -0.25), 0.4375, ((0, 4), (1, 8)))
    log_decay = draw_log_decay(jax.random.fold_in(splits[13], 71), 0)
    out_gate = centred(splits[4], (TOKENS, INNER), 1.0, 6.0, ((0, 4), (1, 8)))
    out_proj = centred(splits[5], (D, INNER), INNER ** -0.5, 0.125, ((1, 8),))
    mixed = centred(splits[6], (TOKENS, D), 1.0, 6.0, ((0, 4),))
    cotangent = gaussian_with(splits[7], (TOKENS, D), 1.0, 8.0, ((0, 4),), (0, 1, 4, 2.0))
    route_ids_keys = jax.random.split(jax.random.fold_in(splits[8], 1), TOKENS // TOK_DEV)
    route_ids_turns = jax.random.permutation(jax.random.fold_in(splits[8], 3), TOKENS // TOK_DEV)
    route_ids = jax.vmap(lambda own, number: deal_out(jax.random.fold_in(splits[8], 2), own, number, TOK_DEV, EXPERTS, TOP, CAP, 2))(route_ids_keys, route_ids_turns).reshape((TOKENS, TOP))
    route_weights = jnp.clip(0.25 + 0.75 * jax.random.uniform(splits[9], (TOKENS, TOP), jnp.float32) ** shard_levels(splits[9], (TOKENS, TOP), ((0, 4),), -0.2, 0.2), 0.25, 1.0)
    w_gate = centred(splits[10], (EXPERTS, D, EXPERT_HIDDEN_SIZE), D ** -0.5, 0.09375, ((0, 4), (2, 8)))
    w_up = centred(splits[11], (EXPERTS, D, EXPERT_HIDDEN_SIZE), D ** -0.5, 0.09375, ((0, 4), (2, 8)))
    w_down = centred(splits[12], (EXPERTS, EXPERT_HIDDEN_SIZE, D), EXPERT_HIDDEN_SIZE ** -0.5, 0.125, ((0, 4), (1, 8)))
    return {"token_values": token_values, "write_keys": write_keys, "read_keys": read_keys, "log_decay": log_decay, "out_gate": out_gate, "out_proj": out_proj, "mixed": mixed, "cotangent": cotangent, "route_ids": route_ids, "route_weights": route_weights, "w_gate": w_gate, "w_up": w_up, "w_down": w_down}


highest = lax.Precision.HIGHEST

def mix_blocks(token_values, write_keys, read_keys, log_decay, entering):
    length = token_values.shape[0]
    heads = log_decay.shape[0]
    groups = write_keys.shape[1] // STATE
    per_group = heads // groups
    blocks = length // BLOCK
    inputs = token_values.reshape(blocks, BLOCK, groups, per_group, HEAD_DIM)
    writes = write_keys.reshape(blocks, BLOCK, groups, STATE)
    reads = read_keys.reshape(blocks, BLOCK, groups, STATE)
    decay = log_decay.reshape(groups, per_group, blocks, BLOCK).transpose(2, 3, 0, 1)
    cumul = jnp.cumsum(decay, axis=1)
    spans = cumul[:, :, None] - cumul[:, None, :]
    position = jnp.arange(BLOCK, dtype=jnp.int32)
    lower = (position[:, None] >= position[None, :])[None, :, :, None, None]
    weights = jnp.exp(jnp.where(lower, spans, -jnp.inf))
    scores = jnp.einsum('clgn,csgn->clsg', reads, writes, precision=highest)
    inner = jnp.einsum('clsgr,csgrp->clgrp', scores[..., None] * weights, inputs, precision=highest)
    tails = jnp.exp(cumul[:, -1:] - cumul)
    block_states = jnp.einsum('clgn,clgrp->cgrpn', writes, inputs * tails[..., None], precision=highest)
    block_decay = jnp.exp(cumul[:, -1])

    def advance(state, pieces):
        factor, added = pieces
        return (factor[..., None, None] * state + added, state)
    final, before = lax.scan(advance, entering.reshape(groups, per_group, HEAD_DIM, STATE), (block_decay, block_states))
    carried = jnp.einsum('clgn,cgrpn->clgrp', reads, before, precision=highest) * jnp.exp(cumul)[..., None]
    return ((inner + carried).reshape(length, heads * HEAD_DIM), final.reshape(heads, HEAD_DIM, STATE))

def expert_pass(pieces):
    rows, scaled, gate_weight, up_weight, down_weight = pieces
    gate_pre = jnp.dot(rows, gate_weight, preferred_element_type=jnp.float32)
    up_pre = jnp.dot(rows, up_weight, preferred_element_type=jnp.float32)
    sigma = jax.nn.sigmoid(gate_pre)
    hidden = (jax.nn.silu(gate_pre) * up_pre).astype(jnp.bfloat16)
    grad_down = jnp.dot(hidden.T, scaled, preferred_element_type=jnp.float32).astype(jnp.bfloat16)
    d_hidden = jnp.dot(scaled, down_weight.T, preferred_element_type=jnp.float32)
    d_gate = (d_hidden * up_pre * sigma * (1.0 + gate_pre * (1.0 - sigma))).astype(jnp.bfloat16)
    d_up = (d_hidden * jax.nn.silu(gate_pre)).astype(jnp.bfloat16)
    grad_gate = jnp.dot(rows.T, d_gate, preferred_element_type=jnp.float32).astype(jnp.bfloat16)
    grad_up = jnp.dot(rows.T, d_up, preferred_element_type=jnp.float32).astype(jnp.bfloat16)
    number = rows.shape[0]
    width = gate_weight.shape[0]
    value_portion = jnp.einsum('rqf,dqf->qrd', d_gate.astype(jnp.float32).reshape(number, N_TP, -1), gate_weight.astype(jnp.float32).reshape(width, N_TP, -1))
    value_portion = value_portion + jnp.einsum('rqf,dqf->qrd', d_up.astype(jnp.float32).reshape(number, N_TP, -1), up_weight.astype(jnp.float32).reshape(width, N_TP, -1))
    rounded = lax.optimization_barrier(value_portion.astype(jnp.bfloat16)).astype(jnp.float32)
    return (grad_gate, grad_up, grad_down, lax.optimization_barrier(jnp.sum(rounded, axis=0)).astype(jnp.bfloat16))

def reference(token_values, write_keys, read_keys, log_decay, out_gate, out_proj, mixed, cotangent, route_ids, route_weights, w_gate, w_up, w_down):
    width = mixed.shape[1]
    flat_ids = route_ids.reshape(-1).astype(jnp.int32)
    pairs = flat_ids.shape[0]
    source = jnp.arange(pairs, dtype=jnp.int32) // (TOP * TOK_DEV)
    member = (flat_ids[:, None] == jnp.arange(EXPERTS, dtype=jnp.int32)[None, :]).astype(jnp.int32)
    blocked = member.reshape(N_SP, TOP * TOK_DEV, EXPERTS)
    earlier = (jnp.cumsum(blocked, axis=1).astype(jnp.int32) - blocked).reshape(pairs, EXPERTS)
    slot_index = lax.optimization_barrier(jnp.sum(earlier * member, axis=1)).astype(jnp.int32)
    target = ((flat_ids * N_SP + source) * CAP + slot_index).astype(jnp.int32)
    copies = jnp.repeat(mixed, TOP, axis=0)
    scaled = (cotangent.astype(jnp.float32)[:, None, :] * route_weights[:, :, None]).reshape(pairs, width)
    scaled = scaled.astype(jnp.bfloat16)
    places = EXPERTS * N_SP * CAP
    incoming_rows = jnp.zeros((places, width), jnp.bfloat16).at[target].set(copies).reshape(EXPERTS, N_SP * CAP, width)
    scaled_in = jnp.zeros((places, width), jnp.bfloat16).at[target].set(scaled).reshape(EXPERTS, N_SP * CAP, width)
    grad_gate, grad_up, grad_down, row_grads = lax.map(expert_pass, (incoming_rows, scaled_in, w_gate, w_up, w_down))
    picked = jnp.take(row_grads.reshape(places, width), target, axis=0).astype(jnp.float32)
    picked = picked.reshape(-1, TOP, width)
    grad_mixed = (cotangent.astype(jnp.float32) + lax.optimization_barrier(jnp.sum(picked, axis=1))).astype(jnp.bfloat16)
    out_grad = jnp.dot(grad_mixed, out_proj, preferred_element_type=jnp.float32)
    entering = jnp.zeros((log_decay.shape[0], HEAD_DIM, STATE), jnp.float32)

    def whole_mix(values_in, writes_in, reads_in, gate_in):
        mixed_heads, final = mix_blocks(values_in, writes_in, reads_in, log_decay, entering)
        return mixed_heads * jax.nn.silu(gate_in)
    gated, pullback = jax.vjp(whole_mix, token_values.astype(jnp.float32), write_keys.astype(jnp.float32), read_keys.astype(jnp.float32), out_gate.astype(jnp.float32))
    d_values, d_writes, d_reads, d_gate = pullback(out_grad)
    gated_b = gated.astype(jnp.bfloat16)
    proj_grad = jnp.dot(grad_mixed.T, gated_b, preferred_element_type=jnp.float32)
    return (d_values.astype(jnp.bfloat16), d_writes.astype(jnp.bfloat16), d_reads.astype(jnp.bfloat16), d_gate.astype(jnp.bfloat16), proj_grad, grad_gate, grad_up, grad_down)
```

```python
import functools

import jax
import jax.numpy as jnp
from jax import lax
from jax.experimental import pallas as pl
from jax.experimental.pallas import tpu as pltpu
from jax.sharding import PartitionSpec as P

HEAD_DIM = 64
STATE = 128

F32 = jnp.float32
BF16 = jnp.bfloat16
MESH = pl.DeviceIdType.MESH


def dot(a, b, ca=1, cb=0):
    return lax.dot_general(a, b, (((ca,), (cb,)), ((), ())), preferred_element_type=F32)


class Links:
    def __init__(self, send_sem, recv_sem):
        self.send_sem, self.recv_sem = send_sem, recv_sem
        self.used = 0
        self.started = []

    def slot(self):
        self.used += 1
        return self.used - 1

    def copy(self, slot, src, dst, device):
        return pltpu.make_async_remote_copy(
            src_ref=src,
            dst_ref=dst,
            send_sem=self.send_sem.at[slot],
            recv_sem=self.recv_sem.at[slot],
            device_id=device,
            device_id_type=MESH,
        )

    def start(self, slot, src, dst, device):
        made = self.copy(slot, src, dst, device)
        made.start()
        self.started.append(made)

    def arrived(self, slot, dst, device):
        self.copy(slot, dst, dst, device).wait_recv()

    def finish(self):
        for made in self.started:
            made.wait_send()


class Spread:
    def __init__(self, links, t, window):
        self.links, self.window = links, window
        self.other, self.across, self.along = ({"tp": t ^ bit} for bit in (1, 2, 4))
        self.slots = [links.slot() for _ in range(9)]

    def send(self, kind, bits, part, device):
        w = self.window(bits, part)
        self.links.start(self.slots[kind], w, w, device)

    def got(self, kind, bits, part, device):
        self.links.arrived(self.slots[kind], self.window(bits, part), device)

    def p0(self):
        self.send(1, 0, None, self.across)
        self.send(2, 0, None, self.along)
        self.send(5, 0, None, self.other)

    def p1(self):
        self.got(1, 2, None, self.across)
        self.send(3, 2, 0, self.along)
        self.send(6, 2, None, self.other)
        self.got(2, 4, None, self.along)
        self.send(4, 4, 1, self.across)
        self.send(7, 4, None, self.other)

    def p2(self):
        self.got(3, 6, 0, self.along)
        self.got(4, 6, 1, self.across)
        self.send(8, 6, None, self.other)

    def p3(self):
        for kind, bits in ((5, 1), (6, 3), (7, 5), (8, 7)):
            self.got(kind, bits, None, self.other)


def greet(n, t, s):
    peers = [{"tp": t ^ bit} for bit in (1, 2, 4)] + [{"sp": s ^ k} for k in range(1, n)]
    barrier = pltpu.get_barrier_semaphore()
    for peer in peers:
        pl.semaphore_signal(barrier, inc=1, device_id=peer, device_id_type=MESH)
    pl.semaphore_wait(barrier, len(peers))


def main_kernel(
    n,
    ranks,
    pieces,
    onehot,
    onehot_t,
    row_weight,
    mixed,
    cotangent,
    w_gate,
    w_up,
    w_down,
    gw_out,
    uw_out,
    dw_out,
    gm_out,
    M,
    C,
    W2,
    WD,
    X,
    S,
    SX,
    SS,
    DGU,
    HID,
    HT,
    PB,
    RB,
    SA,
    RX,
    RY,
    BX,
    BY,
    RX2,
    RY2,
    FIN,
    CB,
    G,
    GW,
    UW,
    DW,
    send_sem,
    recv_sem,
    local_sem,
):
    t = lax.axis_index("tp")
    s = lax.axis_index("sp")
    tok, width = M.shape
    hid = WD.shape[0]
    cap = onehot.shape[0] // n
    share = width // ranks
    half_share = share // 2
    blocks = PB.shape[0]
    group = n // blocks
    R = group * cap
    strip = width // pieces
    pw = strip // ranks
    c = lax.rem(t, 2)
    mx = lax.rem(t // 2, 2)
    my = t // 4
    links = Links(send_sem, recv_sem)
    other, across, along = ({"tp": t ^ bit} for bit in (1, 2, 4))

    def load(i, src, dst):
        made = pltpu.make_async_copy(src, dst, local_sem.at[i])
        made.start()
        return made

    loads = [
        load(0, mixed, M),
        load(1, cotangent, C),
        load(2, w_gate, W2.at[:, pl.ds(0, hid)]),
        load(3, w_up, W2.at[:, pl.ds(hid, hid)]),
        load(4, w_down, WD),
    ]
    greet(n, t, s)
    loads[0].wait()
    loads[1].wait()

    mine = pl.ds(pl.multiple_of(t * share, 128), share)
    z_slots = [[links.slot() for _ in range(n)] for _ in range(2)]
    m_part, c_part = M[:, mine], C[:, mine]
    for k in range(1, n):
        pick = onehot[pl.ds(k * cap, cap), :]
        SX[k - 1] = dot(pick, m_part).astype(BF16)
        SS[k - 1] = (dot(pick, c_part) * row_weight[pl.ds(k * cap, cap), :]).astype(BF16)
        for a, (src, dst) in enumerate(((SX, X), (SS, S))):
            links.start(
                z_slots[a][k], src.at[k - 1], dst.at[pl.ds(k * cap, cap), mine], {"sp": s ^ k}
            )

    def local_rows(i, _):
        at = pl.ds(pl.multiple_of(i * share, 128), share)
        pick = onehot[pl.ds(0, cap), :]
        X[pl.ds(0, cap), at] = dot(pick, M[:, at]).astype(BF16)
        S[pl.ds(0, cap), at] = (dot(pick, C[:, at]) * row_weight[pl.ds(0, cap), :]).astype(BF16)
        return 0

    lax.fori_loop(0, ranks, local_rows, 0)

    chunks = {}
    for q in range(blocks):
        first = cap if q == 0 else 0
        if first == R:
            continue
        for a, ref in enumerate((X, S)):

            def window(bits, part, ref=ref, row=q * R + first, count=R - first):
                begin, size = (t ^ bits) * share, share
                if part is not None:
                    begin, size = begin + part * half_share, half_share
                return ref.at[pl.ds(row, count), pl.ds(pl.multiple_of(begin, 128), size)]

            chunks[(q, a)] = Spread(links, t, window)

    def p0(q, a):
        ref = (X, S)[a]
        for k in range(q * group, (q + 1) * group):
            if k:
                links.arrived(z_slots[a][k], ref.at[pl.ds(k * cap, cap), mine], {"sp": s ^ k})
        chunks[(q, a)].p0()

    def p(stage, q, a):
        getattr(chunks[(q, a)], stage)()

    def expert(q):
        r = pl.ds(q * R, R)
        both = dot(X[r, :], W2[...])
        gate, up = both[:, :hid], both[:, hid:]
        sigma = jax.nn.sigmoid(gate)
        act = gate * sigma
        HID[r, :] = (act * up).astype(BF16)
        d_act = dot(S[r, :], WD[...], 1, 1)
        DGU[r, pl.ds(0, hid)] = (d_act * up * sigma * (1.0 + gate * (1.0 - sigma))).astype(BF16)
        DGU[r, pl.ds(hid, hid)] = (d_act * act).astype(BF16)

    def portion(q):
        r = pl.ds(q * R, R)
        step = 256
        for j in range(pieces):

            def some(i, _, j=j):
                begin = pl.multiple_of(j * strip + i * step, 128)
                tile = dot(DGU[r, :], W2[pl.ds(begin, step), :], 1, 1).astype(BF16)
                if pw >= step:
                    per = pw // step
                    dest, off = i // per, lax.rem(i, per) * step
                    at = pl.ds(pl.multiple_of(j * pw + off, 128), step)
                    PB[q, lax.rem(dest, 2), dest // 2, :, at] = tile
                else:
                    at = pl.ds(j * pw, pw)
                    PB[q, 0, i, :, at] = tile[:, :pw]
                    PB[q, 1, i, :, at] = tile[:, pw:]
                return 0

            lax.fori_loop(0, strip // step, some, 0)

    rs_slots = [[links.slot() for _ in range(5)] for _ in range(blocks)]
    back_slots = [links.slot() for _ in range(n)]
    lo, hi = pl.ds(0, half_share), pl.ds(half_share, half_share)

    def r0(q):
        links.start(rs_slots[q][0], PB.at[q, 1 - c], RB.at[q], other)

    def r1(q):
        links.arrived(rs_slots[q][0], RB.at[q], other)

        def add(i, _):
            SA[q, i // 2, lax.rem(i, 2)] = (PB[q, c, i].astype(F32) + RB[q, i].astype(F32)).astype(BF16)
            return 0

        lax.fori_loop(0, ranks // 2, add, 0)
        links.start(rs_slots[q][1], SA.at[q, :, 1 - mx, :, lo], RX.at[q], across)
        links.start(rs_slots[q][2], SA.at[q, 1 - my, :, :, hi], RY.at[q], along)

    def r2(q):
        links.arrived(rs_slots[q][1], RX.at[q], across)
        for i in range(2):
            BX[q, i] = (SA[q, i, mx, :, lo].astype(F32) + RX[q, i].astype(F32)).astype(BF16)
        links.start(rs_slots[q][3], BX.at[q, 1 - my], RX2.at[q], along)
        links.arrived(rs_slots[q][2], RY.at[q], along)
        for i in range(2):
            BY[q, i] = (SA[q, my, i, :, hi].astype(F32) + RY[q, i].astype(F32)).astype(BF16)
        links.start(rs_slots[q][4], BY.at[q, 1 - mx], RY2.at[q], across)

    def r3(q):
        r = pl.ds(q * R, R)
        links.arrived(rs_slots[q][3], RX2.at[q], along)
        FIN[r, lo] = (BX[q, my].astype(F32) + RX2[q].astype(F32)).astype(BF16)
        links.arrived(rs_slots[q][4], RY2.at[q], across)
        FIN[r, hi] = (BY[q, mx].astype(F32) + RY2[q].astype(F32)).astype(BF16)
        for k in range(q * group, (q + 1) * group):
            rows = pl.ds(k * cap, cap)
            if k:
                links.start(back_slots[k], FIN.at[rows, :], CB.at[rows, :], {"sp": s ^ k})
            else:
                CB[rows, :] = FIN[rows, :]

    def grads_gate_up(first, last):
        def some(i, _):
            at = pl.ds(pl.multiple_of(i * 256, 128), 256)
            tile = dot(X[:, at], DGU[...], 0, 0).astype(BF16)
            GW[at, :] = tile[:, :hid]
            UW[at, :] = tile[:, hid:]
            return 0

        lax.fori_loop(first, last, some, 0)

    def grads_down():
        HT[...] = HID[...].T

        def some(i, _):
            at = pl.ds(pl.multiple_of(i * 512, 128), 512)
            DW[:, at] = dot(HT[...], S[:, at]).astype(BF16)
            return 0

        lax.fori_loop(0, width // 512, some, 0)

    order = [key for key in chunks]
    count = len(order)

    def forward(i):
        if i < count:
            p0(*order[i])
        if 0 <= i - 1 < count:
            p("p1", *order[i - 1])
        if 0 <= i - 2 < count:
            p("p2", *order[i - 2])

    def whole(q):
        for a in range(2):
            if (q, a) in chunks:
                p("p3", q, a)
        expert(q)
        portion(q)
        r0(q)

    for i in range(2, 5):
        loads[i].wait()
    if blocks == 4 and (0, 0) not in chunks:
        forward(0)
        expert(0)
        forward(1)
        portion(0)
        r0(0)
        forward(2)
        r1(0)
        forward(3)
        r2(0)
        forward(4)
        whole(1)
        r3(0)
        forward(5)
        r1(1)
        forward(6)
        whole(2)
        r2(1)
        forward(7)
        r1(2)
        r3(1)
        whole(3)
        r2(2)
        r1(3)
    else:
        for i in range(count + 2):
            forward(i)
        for q in range(blocks):
            whole(q)
        for q in range(blocks):
            r1(q)
        for q in range(blocks - 1):
            r2(q)
        for q in range(blocks - 2):
            r3(q)
    tiles = width // 256
    grads_gate_up(0, tiles // 4)
    r3(blocks - 2)
    r2(blocks - 1)
    grads_gate_up(tiles // 4, tiles // 2)
    r3(blocks - 1)
    grads_gate_up(tiles // 2, tiles)
    outs = [load(5, GW, gw_out), load(6, UW, uw_out)]
    for k in range(1, n):
        rows = pl.ds(k * cap, cap)
        links.arrived(back_slots[k], CB.at[rows, :], {"sp": s ^ k})

    half_tok = tok // 2
    gathers = []
    for i in range(2):

        def window(bits, part, i=i):
            row, rows = i * half_tok, half_tok
            if part is not None:
                row, rows = row + part * (half_tok // 2), half_tok // 2
            return G.at[:, pl.ds(row, rows), pl.ds(pl.multiple_of((t ^ bits) * pw, 128), pw)]

        gathers.append(Spread(links, t, window))
    for i in range(2):
        rows = pl.ds(i * half_tok, half_tok)
        back = dot(onehot_t[rows, :], CB[...])
        for j in range(pieces):
            cot = C[rows, pl.ds(pl.multiple_of(j * strip + t * pw, 128), pw)].astype(F32)
            G[j, rows, pl.ds(pl.multiple_of(t * pw, 128), pw)] = (
                cot + back[:, j * pw : (j + 1) * pw]
            ).astype(BF16)
        gathers[i].p0()
    grads_down()
    outs.append(load(7, DW, dw_out))
    for i in range(2):
        gathers[i].p1()
    for i in range(2):
        gathers[i].p2()
    for i in range(2):
        gathers[i].p3()
    for j in range(pieces):
        outs.append(load(8 + j, G.at[j], gm_out.at[:, pl.ds(j * strip, strip)]))
    links.finish()
    for made in outs:
        made.wait()


def main_call(n, onehot, onehot_t, row_weight, mixed, cotangent, w_gate, w_up, w_down):
    tok, width = mixed.shape
    hid = w_gate.shape[1]
    ranks = lax.axis_size("tp")
    share = width // ranks
    rows = onehot.shape[0]
    cap = rows // n
    pieces = n if (width // n // ranks) % 128 == 0 else 1
    strip = width // pieces
    blocks = 4 if n % 4 == 0 else n
    R = rows // blocks
    slots = 2 * n + 2 * blocks * 9 + 5 * blocks + n + 18
    any_, vmem = pl.BlockSpec(memory_space=pl.ANY), pl.BlockSpec(memory_space=pltpu.VMEM)

    def buf(*shape):
        return pltpu.VMEM(shape, BF16)

    return pl.pallas_call(
        functools.partial(main_kernel, n, ranks, pieces),
        out_shape=[
            jax.ShapeDtypeStruct((width, hid), BF16),
            jax.ShapeDtypeStruct((width, hid), BF16),
            jax.ShapeDtypeStruct((hid, width), BF16),
            jax.ShapeDtypeStruct((tok, width), BF16),
        ],
        in_specs=[vmem] * 3 + [any_] * 5,
        out_specs=[any_] * 4,
        scratch_shapes=[
            buf(tok, width),
            buf(tok, width),
            buf(width, 2 * hid),
            buf(hid, width),
            buf(rows, width),
            buf(rows, width),
            buf(n - 1, cap, share),
            buf(n - 1, cap, share),
            buf(rows, 2 * hid),
            buf(rows, hid),
            buf(hid, rows),
            buf(blocks, 2, ranks // 2, R, share),
            buf(blocks, ranks // 2, R, share),
            buf(blocks, 2, 2, R, share),
            buf(blocks, 2, R, share // 2),
            buf(blocks, 2, R, share // 2),
            buf(blocks, 2, R, share // 2),
            buf(blocks, 2, R, share // 2),
            buf(blocks, R, share // 2),
            buf(blocks, R, share // 2),
            buf(rows, share),
            buf(rows, share),
            buf(pieces, tok, strip),
            buf(width, hid),
            buf(width, hid),
            buf(hid, width),
            pltpu.SemaphoreType.DMA((slots,)),
            pltpu.SemaphoreType.DMA((slots,)),
            pltpu.SemaphoreType.DMA((8 + pieces,)),
        ],
        compiler_params=pltpu.CompilerParams(
            collective_id=1, has_side_effects=True, vmem_limit_bytes=60 * 1024 * 1024
        ),
    )(onehot, onehot_t, row_weight, mixed, cotangent, w_gate, w_up, w_down)


def shift(x, by):
    n = lax.axis_size("sp")
    return lax.ppermute(x, "sp", [(i, (i + by) % n) for i in range(n)])


def spread_kernel(n, arrays, far, *refs):
    sends, outs = refs[:arrays], refs[arrays : 2 * arrays]
    send_sem, recv_sem, local_sem = refs[2 * arrays :]
    t = lax.axis_index("tp")
    s = lax.axis_index("sp")
    blocks, rows, cols = sends[0].shape
    half = rows // 2
    chunks = [(a, j) for a in range(arrays) for j in range(blocks)]
    near = [{"tp": t ^ bit} for bit in (1, 2, 4)]
    other, across, along = near
    peers = list(near)
    if far:
        peers += [{"sp": lax.rem(s + j, n)} for j in range(1, n)]
    barrier = pltpu.get_barrier_semaphore()
    for peer in peers:
        pl.semaphore_signal(barrier, inc=1, device_id=peer, device_id_type=pl.DeviceIdType.MESH)
    pl.semaphore_wait(barrier, len(peers))

    def window(c, bits, start=0, count=rows):
        a, j = chunks[c]
        at = pl.multiple_of((t ^ bits) * cols, 128)
        return outs[a].at[j, pl.ds(start, count), pl.ds(at, cols)]

    def copy(c, kind, src, dst, device):
        return pltpu.make_async_remote_copy(
            src_ref=src,
            dst_ref=dst,
            send_sem=send_sem.at[c, kind],
            recv_sem=recv_sem.at[c, kind],
            device_id=device,
            device_id_type=pl.DeviceIdType.MESH,
        )

    started = []

    def start(*args):
        made = copy(*args)
        made.start()
        started.append(made)

    def arrived(c, kind, dst, device):
        copy(c, kind, dst, dst, device).wait_recv()

    locals_ = []
    for c, (a, j) in enumerate(chunks):
        if far:
            start(c, 0, sends[a].at[j], window(c, 0), {"sp": lax.rem(s + j + 1, n)})
        else:
            made = pltpu.make_async_copy(sends[a].at[j], window(c, 0), local_sem.at[c])
            made.start()
            locals_.append(made)
    total = len(chunks)
    for k in range(total + 2):
        if k < total:
            if far:
                arrived(k, 0, window(k, 0), {"sp": lax.rem(s + 1, n)})
                own = window(k, 0)
            else:
                own = sends[chunks[k][0]].at[chunks[k][1]]
            start(k, 1, own, window(k, 0), across)
            start(k, 2, own, window(k, 0), along)
            start(k, 5, own, window(k, 0), other)
        c = k - 1
        if 0 <= c < total:
            arrived(c, 1, window(c, 2), across)
            start(c, 3, window(c, 2, 0, half), window(c, 2, 0, half), along)
            start(c, 6, window(c, 2), window(c, 2), other)
            arrived(c, 2, window(c, 4), along)
            start(c, 4, window(c, 4, half, rows - half), window(c, 4, half, rows - half), across)
            start(c, 7, window(c, 4), window(c, 4), other)
        c = k - 2
        if 0 <= c < total:
            arrived(c, 3, window(c, 6, 0, half), along)
            arrived(c, 4, window(c, 6, half, rows - half), across)
            start(c, 8, window(c, 6), window(c, 6), other)
    for c in range(total):
        for kind, bits in ((5, 1), (6, 3), (7, 5), (8, 7)):
            arrived(c, kind, window(c, bits), other)
    for made in started:
        made.wait_send()
    for made in locals_:
        made.wait()


def spread(arrays, far, collective_id):
    n = lax.axis_size("sp")
    ranks = lax.axis_size("tp")
    blocks, rows, cols = arrays[0].shape
    count = len(arrays)
    total = count * blocks
    space = pl.ANY if far else pltpu.VMEM
    got = pl.pallas_call(
        functools.partial(spread_kernel, n, count, far),
        out_shape=[jax.ShapeDtypeStruct((blocks, rows, ranks * cols), BF16)] * count,
        in_specs=[pl.BlockSpec(memory_space=space)] * count,
        out_specs=[pl.BlockSpec(memory_space=pl.ANY)] * count,
        scratch_shapes=[
            pltpu.SemaphoreType.DMA((total, 9)),
            pltpu.SemaphoreType.DMA((total, 9)),
            pltpu.SemaphoreType.DMA((total,)),
        ],
        compiler_params=pltpu.CompilerParams(collective_id=collective_id, has_side_effects=True),
    )(*arrays)
    return [g.reshape(blocks * rows, ranks * cols) for g in got]


def body(
    token_values,
    write_keys,
    read_keys,
    log_decay,
    out_gate,
    out_proj,
    mixed,
    cotangent,
    route_ids,
    route_weights,
    w_gate,
    w_up,
    w_down,
):
    tok, width = mixed.shape
    n = lax.axis_size("sp")
    cap = 3 * tok // n
    own = lax.axis_index("sp")

    rel = jnp.bitwise_xor(route_ids, own)
    hit = rel[:, :, None] == jnp.arange(n, dtype=jnp.int32)[None, None, :]
    member = jnp.any(hit, axis=1)
    weight = jnp.sum(jnp.where(hit, route_weights[:, :, None], 0.0), axis=1)
    order = jnp.arange(tok, dtype=jnp.int32)
    before = (order[:, None] > order[None, :]).astype(BF16)
    slot = dot(before, member.astype(BF16)).astype(jnp.int32)
    slot = jnp.where(member, slot, -1).T
    place = jnp.arange(cap, dtype=jnp.int32)
    chosen = slot[:, None, :] == place[None, :, None]
    onehot = chosen.astype(BF16).reshape(n * cap, tok)
    row_weight = jnp.sum(jnp.where(chosen, weight.T[:, None, :], 0.0), axis=2).reshape(n * cap, 1)
    grad_gate, grad_up, grad_down, grad_mixed = main_call(
        n, onehot, onehot.T, row_weight, mixed, cotangent, w_gate[0], w_up[0], w_down[0]
    )

    heads = log_decay.shape[0]
    groups = write_keys.shape[1] // STATE
    per_group = heads // groups
    cumul = jnp.cumsum(log_decay, axis=1)
    total = cumul[:, -1]
    tails = jnp.exp(total[:, None] - cumul)
    leads = jnp.exp(cumul)
    values = token_values.astype(F32)
    gate = out_gate.astype(F32)
    sig = jax.nn.sigmoid(gate)
    silu = gate * sig
    causal = order[:, None] >= order[None, :]

    def widen(per_head):
        return jnp.repeat(per_head.T, HEAD_DIM, axis=1)

    tails_wide = widen(tails)
    leads_wide = widen(leads)
    tailed = (values * tails_wide).astype(BF16)

    def cols(a, g):
        k = per_group * HEAD_DIM
        return a[:, g * k : (g + 1) * k]

    def keys(a, g):
        return a[:, g * STATE : (g + 1) * STATE]

    def head(a, h):
        return a[:, h * HEAD_DIM : (h + 1) * HEAD_DIM]

    local_end = jnp.concatenate(
        [dot(cols(tailed, g), keys(write_keys, g), 0, 0) for g in range(groups)], axis=0
    )
    packed = jnp.concatenate(
        [local_end, jnp.broadcast_to(total[:, None], (heads, STATE))], axis=0
    ).astype(BF16)
    lengths = heads * HEAD_DIM
    entering = jnp.zeros((lengths, STATE), F32)
    run = jnp.zeros((heads,), F32)
    for j in range(1, n):
        got = shift(packed, j).astype(F32)
        live = own >= j
        factor = jnp.where(live, jnp.exp(run), 0.0)
        entering = entering + jnp.repeat(factor, HEAD_DIM)[:, None] * got[:lengths]
        run = run + jnp.where(live, got[lengths:, 0], 0.0)
    ahead = [shift(packed[lengths:], -j).astype(F32)[:, 0] for j in range(1, n)]
    entering_b = entering.astype(BF16)

    decay_of, kept, outs = [], [], []
    scores = [dot(keys(read_keys, g), keys(write_keys, g), 1, 1) for g in range(groups)]
    for h in range(heads):
        span = cumul[h][:, None] - cumul[h][None, :]
        decay = jnp.exp(jnp.where(causal, span, -jnp.inf))
        decay_of.append(decay)
        kept.append((scores[h // per_group] * decay).astype(BF16))
        outs.append(dot(kept[h], head(token_values, h)))
    carried = jnp.concatenate(
        [
            dot(keys(read_keys, g), entering_b[g * per_group * HEAD_DIM : (g + 1) * per_group * HEAD_DIM], 1, 1)
            for g in range(groups)
        ],
        axis=1,
    )
    y = jnp.concatenate(outs, axis=1) + carried * leads_wide
    gated_b = (y * silu).astype(BF16)

    out_grad = dot(grad_mixed, out_proj)
    quarter = width // n
    piece = quarter // lax.axis_size("tp")
    lane = lax.axis_index("tp") * piece
    if piece % 128 == 0:
        send_mixed = jnp.stack(
            [
                lax.dynamic_slice_in_dim(grad_mixed, lax.rem(own + j, n) * quarter + lane, piece, 1)
                for j in range(1, n)
            ]
        )
        (far_mixed,) = spread([send_mixed], True, 3)
        own_mixed = lax.dynamic_slice_in_dim(grad_mixed, own * quarter, quarter, 1)
        far_gated = jnp.concatenate([shift(gated_b, j) for j in range(1, n)], axis=0)
        proj_grad = dot(own_mixed, gated_b, 0, 0) + dot(far_mixed, far_gated, 0, 0)
    else:
        proj_part = dot(grad_mixed, gated_b, 0, 0).astype(BF16)
        proj_grad = lax.psum_scatter(proj_part, "sp", scatter_dimension=0, tiled=True).astype(F32)

    outer = out_grad * silu
    outer_b = outer.astype(BF16)
    led = (outer * leads_wide).astype(BF16)
    local_back = jnp.concatenate(
        [dot(cols(led, g), keys(read_keys, g), 0, 0) for g in range(groups)], axis=0
    ).astype(BF16)
    leaving = jnp.zeros((lengths, STATE), F32)
    run = jnp.zeros((heads,), F32)
    for j in range(1, n):
        got = shift(local_back, -j).astype(F32)
        live = own + j < n
        factor = jnp.where(live, jnp.exp(run), 0.0)
        leaving = leaving + jnp.repeat(factor, HEAD_DIM)[:, None] * got
        run = run + jnp.where(live, ahead[j - 1], 0.0)
    leaving_b = leaving.astype(BF16)

    d_values, d_writes, d_reads = [], [], []
    for g in range(groups):
        d_scores = 0.0
        for r in range(per_group):
            h = g * per_group + r
            d_scores = d_scores + dot(head(outer_b, h), head(token_values, h), 1, 1) * decay_of[h]
            d_values.append(dot(kept[h], head(outer_b, h), 0, 0))
        d_scores = d_scores.astype(BF16)
        span = slice(g * per_group * HEAD_DIM, (g + 1) * per_group * HEAD_DIM)
        d_reads.append(dot(d_scores, keys(write_keys, g)) + dot(led[:, span], entering_b[span]))
        d_writes.append(
            dot(d_scores, keys(read_keys, g), 0, 0) + dot(tailed[:, span], leaving_b[span])
        )
    from_end = jnp.concatenate(
        [
            dot(keys(write_keys, g), leaving_b[g * per_group * HEAD_DIM : (g + 1) * per_group * HEAD_DIM], 1, 1)
            for g in range(groups)
        ],
        axis=1,
    )
    d_values = jnp.concatenate(d_values, axis=1) + from_end * tails_wide
    d_out_gate = out_grad * y * sig * (1.0 + gate * (1.0 - sig))
    return (
        d_values.astype(BF16),
        jnp.concatenate(d_writes, axis=1).astype(BF16),
        jnp.concatenate(d_reads, axis=1).astype(BF16),
        d_out_gate.astype(BF16),
        proj_grad,
        grad_gate[None],
        grad_up[None],
        grad_down[None],
    )


def solution(mesh):
    return jax.shard_map(
        body,
        mesh=mesh,
        in_specs=(
            P("sp", "tp"),
            P("sp", "tp"),
            P("sp", "tp"),
            P("tp", "sp"),
            P("sp", "tp"),
            P(None, "tp"),
            P("sp", None),
            P("sp", None),
            P("sp", None),
            P("sp", None),
            P("sp", None, "tp"),
            P("sp", None, "tp"),
            P("sp", "tp", None),
        ),
        out_specs=(
            P("sp", "tp"),
            P("sp", "tp"),
            P("sp", "tp"),
            P("sp", "tp"),
            P("sp", "tp"),
            P("sp", None, "tp"),
            P("sp", None, "tp"),
            P("sp", "tp", None),
        ),
        check_vma=False,
    )
```

```python
import functools

import jax
import jax.numpy as jnp
from jax import lax
from jax.experimental import pallas as pl
from jax.experimental.pallas import tpu as pltpu
from jax.sharding import PartitionSpec as P

HEAD_DIM = 64
STATE = 128

F32 = jnp.float32
BF16 = jnp.bfloat16
MESH = pl.DeviceIdType.MESH


def dot(a, b, ca=1, cb=0):
    return lax.dot_general(a, b, (((ca,), (cb,)), ((), ())), preferred_element_type=F32)


class Links:
    def __init__(self, send_sem, recv_sem):
        self.send_sem, self.recv_sem = send_sem, recv_sem
        self.used = 0
        self.started = []

    def slot(self):
        self.used += 1
        return self.used - 1

    def copy(self, slot, src, dst, device):
        return pltpu.make_async_remote_copy(
            src_ref=src,
            dst_ref=dst,
            send_sem=self.send_sem.at[slot],
            recv_sem=self.recv_sem.at[slot],
            device_id=device,
            device_id_type=MESH,
        )

    def start(self, slot, src, dst, device):
        made = self.copy(slot, src, dst, device)
        made.start()
        self.started.append(made)

    def arrived(self, slot, dst, device):
        self.copy(slot, dst, dst, device).wait_recv()

    def finish(self):
        for made in self.started:
            made.wait_send()


class Spread:
    def __init__(self, links, t, window):
        self.links, self.window = links, window
        self.other, self.across, self.along = ({"tp": t ^ bit} for bit in (1, 2, 4))
        self.slots = [links.slot() for _ in range(9)]

    def send(self, kind, bits, part, device):
        w = self.window(bits, part)
        self.links.start(self.slots[kind], w, w, device)

    def got(self, kind, bits, part, device):
        self.links.arrived(self.slots[kind], self.window(bits, part), device)

    def p0(self):
        self.send(1, 0, None, self.across)
        self.send(2, 0, None, self.along)
        self.send(5, 0, None, self.other)

    def p1(self):
        self.got(1, 2, None, self.across)
        self.send(3, 2, 0, self.along)
        self.send(6, 2, None, self.other)
        self.got(2, 4, None, self.along)
        self.send(4, 4, 1, self.across)
        self.send(7, 4, None, self.other)

    def p2(self):
        self.got(3, 6, 0, self.along)
        self.got(4, 6, 1, self.across)
        self.send(8, 6, None, self.other)

    def p3(self):
        for kind, bits in ((5, 1), (6, 3), (7, 5), (8, 7)):
            self.got(kind, bits, None, self.other)


def greet(n, t, s):
    peers = [{"tp": t ^ bit} for bit in (1, 2, 4)] + [{"sp": s ^ k} for k in range(1, n)]
    barrier = pltpu.get_barrier_semaphore()
    for peer in peers:
        pl.semaphore_signal(barrier, inc=1, device_id=peer, device_id_type=MESH)
    pl.semaphore_wait(barrier, len(peers))


def main_kernel(
    n,
    ranks,
    pieces,
    ids_in,
    weights_in,
    mixed,
    cotangent,
    w_gate,
    w_up,
    w_down,
    values_in,
    writes_in,
    reads_in,
    decay_in,
    gate_in,
    proj_in,
    value_out,
    write_out,
    read_out,
    gate_out,
    *refs,
):
    outs_proj = refs[: 1 if pieces == n else 2]
    gw_out, uw_out, dw_out = refs[len(outs_proj) : len(outs_proj) + 3]
    (
        IDS, RW, M, C, W2, WD, X, S, SX, SS, ONE, WCOL, DGU, HID, HT,
        PB, RB, RX, RY, RX2, RY2, FIN, CB, G, GW, UW, DW,
        TV, WK, RK, LD, OGT, OP, LW, TW, Y, DEC, KT, TLD, END, TOT, BK, ENT, GB, F,
        OG, OB, LED, DWF, DV, DWK, DRK, DGT, PJ,
        send_sem, recv_sem, local_sem,
    ) = refs[len(outs_proj) + 3 :]
    t = lax.axis_index("tp")
    s = lax.axis_index("sp")
    tok, width = M.shape
    hid = WD.shape[0]
    cap = CB.shape[0] // n
    share = width // ranks
    half_share = share // 2
    blocks = PB.shape[0]
    group = n // blocks
    R = group * cap
    strip = width // pieces
    pw = strip // ranks
    heads = LD.shape[0]
    groups = WK.shape[1] // STATE
    per_group = heads // groups
    chan = per_group * HEAD_DIM
    c = lax.rem(t, 2)
    mx = lax.rem(t // 2, 2)
    my = t // 4
    links = Links(send_sem, recv_sem)
    other, across, along = ({"tp": t ^ bit} for bit in (1, 2, 4))
    loaded = [0]

    def load(src, dst):
        made = pltpu.make_async_copy(src, dst, local_sem.at[loaded[0]])
        loaded[0] += 1
        made.start()
        return made

    first_loads = [load(ids_in, IDS), load(weights_in, RW), load(mixed, M), load(cotangent, C)]
    mix_loads = [
        load(decay_in, LD),
        load(writes_in, WK),
        load(values_in, TV),
        load(reads_in, RK),
        load(gate_in, OGT),
    ]
    expert_loads = [
        load(w_gate, W2.at[:, pl.ds(0, hid)]),
        load(w_up, W2.at[:, pl.ds(hid, hid)]),
        load(w_down, WD),
    ]
    proj_load = load(proj_in, OP)
    greet(n, t, s)
    for made in first_loads:
        made.wait()

    rows_n = max(n, 8)
    lane = lax.broadcasted_iota(jnp.int32, (rows_n, tok), 0) ^ s
    names = [IDS[i : i + 1, :] == lane for i in range(IDS.shape[0])]
    member = functools.reduce(jnp.logical_or, names)
    weight = sum(jnp.where(names[i], RW[i : i + 1, :], 0.0) for i in range(IDS.shape[0]))
    row_of = lax.broadcasted_iota(jnp.int32, (tok, tok), 0)
    col_of = lax.broadcasted_iota(jnp.int32, (tok, tok), 1)
    earlier = (row_of < col_of).astype(F32).astype(BF16)
    slot = dot(member.astype(F32).astype(BF16), earlier)
    slot = jnp.where(member, slot, -1.0).astype(jnp.int32)
    place = lax.broadcasted_iota(jnp.int32, (cap, tok), 0)

    mine = pl.ds(pl.multiple_of(t * share, 128), share)
    z_slots = [[links.slot() for _ in range(n)] for _ in range(2)]
    m_part, c_part = M[:, mine], C[:, mine]
    for k in list(range(1, n)) + [0]:
        rows = pl.ds(k * cap, cap)
        chosen = slot[k : k + 1, :] == place
        pick = chosen.astype(F32).astype(BF16)
        row_weight = jnp.sum(jnp.where(chosen, weight[k : k + 1, :], 0.0), axis=1, keepdims=True)
        ONE[rows, :] = pick
        if k:
            SX[k - 1] = dot(pick, m_part).astype(BF16)
            SS[k - 1] = (dot(pick, c_part) * row_weight).astype(BF16)
            for a, (src, dst) in enumerate(((SX, X), (SS, S))):
                links.start(z_slots[a][k], src.at[k - 1], dst.at[rows, mine], {"sp": s ^ k})
        else:
            WCOL[...] = jnp.broadcast_to(row_weight, WCOL.shape)

    def local_rows():
        def some(i, _):
            at = pl.ds(pl.multiple_of(i * share, 128), share)
            pick = ONE[pl.ds(0, cap), :]
            X[pl.ds(0, cap), at] = dot(pick, M[:, at]).astype(BF16)
            S[pl.ds(0, cap), at] = (dot(pick, C[:, at]) * WCOL[:, :1]).astype(BF16)
            return 0

        lax.fori_loop(0, ranks, some, 0)

    chunks = {}
    for q in range(blocks):
        first = cap if q == 0 else 0
        if first == R:
            continue
        for a, ref in enumerate((X, S)):

            def window(bits, part, ref=ref, row=q * R + first, count=R - first):
                begin, size = (t ^ bits) * share, share
                if part is not None:
                    begin, size = begin + part * half_share, half_share
                return ref.at[pl.ds(row, count), pl.ds(pl.multiple_of(begin, 128), size)]

            chunks[(q, a)] = Spread(links, t, window)

    def p0(q, a):
        ref = (X, S)[a]
        for k in range(q * group, (q + 1) * group):
            if k:
                links.arrived(z_slots[a][k], ref.at[pl.ds(k * cap, cap), mine], {"sp": s ^ k})
        chunks[(q, a)].p0()

    def expert(q):
        r = pl.ds(q * R, R)
        both = dot(X[r, :], W2[...])
        gate, up = both[:, :hid], both[:, hid:]
        sigma = jax.nn.sigmoid(gate)
        act = gate * sigma
        HID[r, :] = (act * up).astype(BF16)
        d_act = dot(S[r, :], WD[...], 1, 1)
        DGU[r, pl.ds(0, hid)] = (d_act * up * sigma * (1.0 + gate * (1.0 - sigma))).astype(BF16)
        DGU[r, pl.ds(hid, hid)] = (d_act * act).astype(BF16)

    def portion(q):
        r = pl.ds(q * R, R)
        step = 256
        for j in range(pieces):

            def some(i, _, j=j):
                begin = pl.multiple_of(j * strip + i * step, 128)
                tile = dot(DGU[r, :], W2[pl.ds(begin, step), :], 1, 1).astype(BF16)
                if pw >= step:
                    per = pw // step
                    dest, off = i // per, lax.rem(i, per) * step
                    at = pl.ds(pl.multiple_of(j * pw + off, 128), step)
                    PB[q, lax.rem(dest, 2), dest // 4, lax.rem(dest // 2, 2), :, at] = tile
                else:
                    at = pl.ds(j * pw, pw)
                    PB[q, 0, i // 2, lax.rem(i, 2), :, at] = tile[:, :pw]
                    PB[q, 1, i // 2, lax.rem(i, 2), :, at] = tile[:, pw:]
                return 0

            lax.fori_loop(0, strip // step, some, 0)

    rs_slots = [[links.slot() for _ in range(5)] for _ in range(blocks)]
    back_slots = [links.slot() for _ in range(n)]
    lo, hi = pl.ds(0, half_share), pl.ds(half_share, half_share)

    def r0(q):
        links.start(rs_slots[q][0], PB.at[q, 1 - c], RB.at[q], other)

    def r1(q):
        links.arrived(rs_slots[q][0], RB.at[q], other)

        def add(i, _):
            a, b = i // 2, lax.rem(i, 2)
            RB[q, a, b] = (PB[q, c, a, b].astype(F32) + RB[q, a, b].astype(F32)).astype(BF16)
            return 0

        lax.fori_loop(0, ranks // 2, add, 0)
        links.start(rs_slots[q][1], RB.at[q, :, 1 - mx, :, lo], RX.at[q], across)
        links.start(rs_slots[q][2], RB.at[q, 1 - my, :, :, hi], RY.at[q], along)

    def r2(q):
        links.arrived(rs_slots[q][1], RX.at[q], across)
        for i in range(2):
            RX[q, i] = (RB[q, i, mx, :, lo].astype(F32) + RX[q, i].astype(F32)).astype(BF16)
        links.start(rs_slots[q][3], RX.at[q, 1 - my], RX2.at[q], along)
        links.arrived(rs_slots[q][2], RY.at[q], along)
        for i in range(2):
            RY[q, i] = (RB[q, my, i, :, hi].astype(F32) + RY[q, i].astype(F32)).astype(BF16)
        links.start(rs_slots[q][4], RY.at[q, 1 - mx], RY2.at[q], across)

    def r3(q):
        r = pl.ds(q * R, R)
        links.arrived(rs_slots[q][3], RX2.at[q], along)
        FIN[r, lo] = (RX[q, my].astype(F32) + RX2[q].astype(F32)).astype(BF16)
        links.arrived(rs_slots[q][4], RY2.at[q], across)
        FIN[r, hi] = (RY[q, mx].astype(F32) + RY2[q].astype(F32)).astype(BF16)
        for k in range(q * group, (q + 1) * group):
            rows = pl.ds(k * cap, cap)
            if k:
                links.start(back_slots[k], FIN.at[rows, :], CB.at[rows, :], {"sp": s ^ k})
            else:
                CB[rows, :] = FIN[rows, :]

    def grads_gate_up(first, last):
        def some(i, _):
            at = pl.ds(pl.multiple_of(i * 256, 128), 256)
            tile = dot(X[:, at], DGU[...], 0, 0).astype(BF16)
            GW[at, :] = tile[:, :hid]
            UW[at, :] = tile[:, hid:]
            return 0

        lax.fori_loop(first, last, some, 0)

    def grads_down():
        HT[...] = HID[...].T

        def some(i, _):
            at = pl.ds(pl.multiple_of(i * 512, 128), 512)
            DW[:, at] = dot(HT[...], S[:, at]).astype(BF16)
            return 0

        lax.fori_loop(0, width // 512, some, 0)

    head_of = lax.broadcasted_iota(jnp.int32, (tok, chan), 1) // HEAD_DIM
    end_slots = [[links.slot() for _ in range(n)] for _ in range(2)]
    gated_slots = [links.slot() for _ in range(n)]
    state_slots = [links.slot() for _ in range(n)]

    def keys(ref, g):
        return ref[:, g * STATE : (g + 1) * STATE]

    def wide(columns):
        return jnp.concatenate(
            [jnp.broadcast_to(columns[:, h : h + 1], (tok, HEAD_DIM)) for h in range(heads)], axis=1
        )

    def everyone(slots, src, dst):
        for k in range(1, n):
            links.start(slots[k], src, dst(k), {"sp": s ^ k})

    def mixer_ends():
        for made in mix_loads:
            made.wait()
        pad = max(heads, 8) - heads
        decays = LD[...]
        if pad:
            decays = jnp.concatenate([decays, jnp.zeros((pad, tok), F32)], axis=0)
        upto = (row_of <= col_of).astype(F32)
        cumul = lax.dot_general(
            decays,
            upto,
            (((1,), (0,)), ((), ())),
            precision=lax.Precision.HIGHEST,
            preferred_element_type=F32,
        )
        total = cumul[:, tok - 1 :]
        TOT[s] = jnp.broadcast_to(total, TOT.shape[1:])
        columns = cumul.T
        spread = wide(columns)
        LW[...] = jnp.exp(spread)
        tails = jnp.exp(spread[tok - 1 :, :] - spread)
        TW[...] = tails
        TLD[...] = (TV[...].astype(F32) * tails).astype(BF16)
        for g in range(groups):
            at = pl.ds(g * chan, chan)
            END[s, at, :] = dot(TLD[:, at], keys(WK, g), 0, 0).astype(BF16)
        everyone(end_slots[0], END.at[s], lambda k: END.at[s])
        everyone(end_slots[1], TOT.at[s], lambda k: TOT.at[s])
        for h in range(heads):
            span = columns[:, h : h + 1] - cumul[h : h + 1, :]
            DEC[h] = jnp.exp(jnp.where(row_of >= col_of, span, -jnp.inf))

    def mixer_inner():
        for g in range(groups):
            scores = dot(keys(RK, g), keys(WK, g), 1, 1)
            at = pl.ds(g * chan, chan)
            inner = jnp.zeros((tok, chan), F32)
            for r in range(per_group):
                h = g * per_group + r
                kept = scores * DEC[h]
                KT[h] = kept.T.astype(BF16)
                inner = jnp.where(head_of == r, dot(kept.astype(BF16), TV[:, at]), inner)
            Y[:, at] = inner

    def factor(j):
        return jnp.concatenate(
            [jnp.broadcast_to(jnp.exp(TOT[j][h : h + 1, :]), (HEAD_DIM, STATE)) for h in range(heads)],
            axis=0,
        )

    def mixer_gated():
        for k in range(1, n):
            links.arrived(end_slots[0][k], END.at[s ^ k], {"sp": s ^ k})
            links.arrived(end_slots[1][k], TOT.at[s ^ k], {"sp": s ^ k})
        state = jnp.zeros(END.shape[1:], F32)
        for j in range(n - 1):
            state = jnp.where(j < s, factor(j) * state + END[j].astype(F32), state)
        ENT[...] = state.astype(BF16)
        for g in range(groups):
            at = pl.ds(g * chan, chan)
            carried = dot(keys(RK, g), ENT[at, :], 1, 1)
            y = Y[:, at] + carried * LW[:, at]
            Y[:, at] = y
            gate = OGT[:, at].astype(F32)
            GB[pl.ds(0, tok), at] = (y * (gate * jax.nn.sigmoid(gate))).astype(BF16)
        if pieces == n:
            own = GB.at[pl.ds(0, tok), :]
            everyone(gated_slots, own, lambda k: GB.at[pl.ds(k * tok, tok), :])

    def mixer_states():
        for g in range(groups):
            at = pl.ds(g * chan, chan)
            gate = OGT[:, at].astype(F32)
            sig = jax.nn.sigmoid(gate)
            outer = OG[:, at] * (gate * sig)
            OB[:, at] = outer.astype(BF16)
            LED[:, at] = (outer * LW[:, at]).astype(BF16)
            BK[s, at, :] = dot(LED[:, at], keys(RK, g), 0, 0).astype(BF16)
        everyone(state_slots, BK.at[s], lambda k: BK.at[s])

    def mixer_scores():
        for g in range(groups):
            at = pl.ds(g * chan, chan)
            gate = OGT[:, at].astype(F32)
            sig = jax.nn.sigmoid(gate)
            DGT[:, at] = (OG[:, at] * Y[:, at] * sig * (1.0 + gate * (1.0 - sig))).astype(BF16)
            d_scores = jnp.zeros((tok, tok), F32)
            d_values = jnp.zeros((tok, chan), F32)
            for r in range(per_group):
                h = g * per_group + r
                one = jnp.where(head_of == r, OB[:, at].astype(F32), 0.0).astype(BF16)
                d_scores = d_scores + dot(one, TV[:, at], 1, 1) * DEC[h]
                d_values = jnp.where(head_of == r, dot(KT[h], OB[:, at]), d_values)
            OG[:, at] = d_values
            d_scores = d_scores.astype(BF16)
            ks = pl.ds(g * STATE, STATE)
            DRK[:, ks] = (dot(d_scores, keys(WK, g)) + dot(LED[:, at], ENT[at, :])).astype(BF16)
            DWF[:, ks] = dot(d_scores, keys(RK, g), 0, 0)

    def mixer_last():
        for k in range(1, n):
            links.arrived(state_slots[k], BK.at[s ^ k], {"sp": s ^ k})
        state = jnp.zeros(BK.shape[1:], F32)
        for j in range(n - 1, 0, -1):
            state = jnp.where(j > s, factor(j) * state + BK[j].astype(F32), state)
        leaving = state.astype(BF16)
        for g in range(groups):
            at = pl.ds(g * chan, chan)
            ks = pl.ds(g * STATE, STATE)
            mine_of = leaving[g * chan : (g + 1) * chan]
            DWK[:, ks] = (DWF[:, ks] + dot(TLD[:, at], mine_of)).astype(BF16)
            d_values = OG[:, at] + dot(keys(WK, g), mine_of, 1, 1) * TW[:, at]
            DV[:, at] = d_values.astype(BF16)

    order = [key for key in chunks]
    count = len(order)

    def forward(i):
        if i < count:
            p0(*order[i])
        if 0 <= i - 1 < count:
            chunks[order[i - 1]].p1()
        if 0 <= i - 2 < count:
            chunks[order[i - 2]].p2()

    def whole(q):
        for a in range(2):
            if (q, a) in chunks:
                chunks[(q, a)].p3()
        expert(q)
        portion(q)
        r0(q)

    mixer_ends()
    local_rows()
    for made in expert_loads:
        made.wait()
    if blocks == 4 and (0, 0) not in chunks:
        forward(0)
        expert(0)
        forward(1)
        portion(0)
        r0(0)
        forward(2)
        r1(0)
        mixer_inner()
        forward(3)
        r2(0)
        mixer_gated()
        forward(4)
        whole(1)
        r3(0)
        forward(5)
        r1(1)
        forward(6)
        whole(2)
        r2(1)
        forward(7)
        r1(2)
        r3(1)
        whole(3)
        r2(2)
        r1(3)
    else:
        mixer_inner()
        mixer_gated()
        for i in range(count + 2):
            forward(i)
        for q in range(blocks):
            whole(q)
        for q in range(blocks):
            r1(q)
        for q in range(blocks - 1):
            r2(q)
        for q in range(blocks - 2):
            r3(q)
    tiles = width // 256
    grads_gate_up(0, tiles // 4)
    r3(blocks - 2)
    r2(blocks - 1)
    grads_gate_up(tiles // 4, tiles // 2)
    r3(blocks - 1)
    grads_gate_up(tiles // 2, tiles)
    outs = [load(GW, gw_out), load(UW, uw_out)]
    for k in range(1, n):
        rows = pl.ds(k * cap, cap)
        links.arrived(back_slots[k], CB.at[rows, :], {"sp": s ^ k})

    half_tok = tok // 2
    gathers = []
    for i in range(2):

        def window(bits, part, i=i):
            row, rows = i * half_tok, half_tok
            if part is not None:
                row, rows = row + part * (half_tok // 2), half_tok // 2
            return G.at[:, pl.ds(row, rows), pl.ds(pl.multiple_of((t ^ bits) * pw, 128), pw)]

        gathers.append(Spread(links, t, window))
    here = pl.ds(pl.multiple_of(t * pw, 128), pw)
    back = dot(ONE[...], CB[...], 0, 0)
    for i in range(2):
        rows = pl.ds(i * half_tok, half_tok)
        for j in range(pieces):
            cot = C[rows, pl.ds(pl.multiple_of(j * strip + t * pw, 128), pw)].astype(F32)
            part = back[i * half_tok : (i + 1) * half_tok, j * pw : (j + 1) * pw]
            G[j, rows, here] = (cot + part).astype(BF16)
        gathers[i].p0()

    fars = []
    if pieces == n:
        far_slots = [links.slot() for _ in range(n)]
        for k in range(1, n):
            rows = pl.ds((k - 1) * tok, tok)
            links.start(far_slots[k], G.at[s ^ k, :, here], F.at[rows, here], {"sp": s ^ k})

            def window(bits, part, k=k):
                row, rows = (k - 1) * tok, tok
                if part is not None:
                    row, rows = row + part * half_tok, half_tok
                return F.at[pl.ds(row, rows), pl.ds(pl.multiple_of((t ^ bits) * pw, 128), pw)]

            fars.append(Spread(links, t, window))

    def far_p0(k):
        rows = pl.ds((k - 1) * tok, tok)
        links.arrived(far_slots[k], F.at[rows, here], {"sp": s ^ k})
        fars[k - 1].p0()

    grads_down()
    outs.append(load(DW, dw_out))
    for i in range(2):
        gathers[i].p1()
    for k in range(1, len(fars) + 1):
        far_p0(k)
    for i in range(2):
        gathers[i].p2()
    for i in range(2):
        gathers[i].p3()
    proj_load.wait()
    OG[...] = sum(dot(G[j], OP[pl.ds(j * strip, strip), :]) for j in range(pieces))
    mixer_states()
    for far in fars:
        far.p1()
    mixer_scores()
    outs.append(load(DGT, gate_out))
    outs.append(load(DRK, read_out))
    for far in fars:
        far.p2()

    def proj_own(i, _):
        at = pl.ds(pl.multiple_of(i * 256, 128), 256)
        PJ[at, :] = dot(G[s, :, at], GB[pl.ds(0, tok), :], 0, 0)
        return 0

    def proj_far(i, _):
        at = pl.ds(pl.multiple_of(i * 256, 128), 256)
        PJ[at, :] += dot(F[:, at], GB[pl.ds(tok, (n - 1) * tok), :], 0, 0)
        return 0

    if pieces == n:
        lax.fori_loop(0, strip // 256, proj_own, 0)
    mixer_last()
    outs.append(load(DWK, write_out))
    outs.append(load(DV, value_out))
    if pieces == n:
        for far in fars:
            far.p3()
        for k in range(1, n):
            links.arrived(gated_slots[k], GB.at[pl.ds(k * tok, tok), :], {"sp": s ^ k})
        lax.fori_loop(0, strip // 256, proj_far, 0)
        outs.append(load(PJ, outs_proj[0]))
    else:
        for j in range(pieces):
            outs.append(load(G.at[j], outs_proj[0].at[:, pl.ds(j * strip, strip)]))
        outs.append(load(GB.at[pl.ds(0, tok), :], outs_proj[1]))
    links.finish()
    for made in outs:
        made.wait()


def body(
    token_values,
    write_keys,
    read_keys,
    log_decay,
    out_gate,
    out_proj,
    mixed,
    cotangent,
    route_ids,
    route_weights,
    w_gate,
    w_up,
    w_down,
):
    tok, width = mixed.shape
    n = lax.axis_size("sp")
    ranks = lax.axis_size("tp")
    hid = w_gate.shape[2]
    inner = token_values.shape[1]
    heads = log_decay.shape[0]
    share = width // ranks
    cap = 3 * tok // n
    rows = n * cap
    pieces = n if (width // n // ranks) % 128 == 0 else 1
    far = pieces == n
    strip = width // pieces
    blocks = 4 if n % 4 == 0 else n
    R = rows // blocks
    slots = 2 * n + 2 * blocks * 9 + 5 * blocks + 6 * n + 18 + 9 * n
    any_ = pl.BlockSpec(memory_space=pl.ANY)

    def buf(*shape, dtype=BF16):
        return pltpu.VMEM(shape, dtype)

    def like(a):
        return jax.ShapeDtypeStruct(a.shape, a.dtype)

    if far:
        proj_shapes = [jax.ShapeDtypeStruct((strip, inner), F32)]
    else:
        proj_shapes = [jax.ShapeDtypeStruct((tok, width), BF16), jax.ShapeDtypeStruct((tok, inner), BF16)]
    operands = [
        route_ids.T,
        route_weights.T,
        mixed,
        cotangent,
        w_gate[0],
        w_up[0],
        w_down[0],
        token_values,
        write_keys,
        read_keys,
        log_decay,
        out_gate,
        out_proj,
    ]
    outputs = (
        [like(token_values), like(write_keys), like(read_keys), like(out_gate)]
        + proj_shapes
        + [like(w_gate[0]), like(w_up[0]), like(w_down[0])]
    )
    got = pl.pallas_call(
        functools.partial(main_kernel, n, ranks, pieces),
        out_shape=outputs,
        in_specs=[any_] * len(operands),
        out_specs=[any_] * len(outputs),
        scratch_shapes=[
            buf(*route_ids.T.shape, dtype=jnp.int32),
            buf(*route_ids.T.shape, dtype=F32),
            buf(tok, width),
            buf(tok, width),
            buf(width, 2 * hid),
            buf(hid, width),
            buf(rows, width),
            buf(rows, width),
            buf(n - 1, cap, share),
            buf(n - 1, cap, share),
            buf(rows, tok),
            buf(cap, 128, dtype=F32),
            buf(rows, 2 * hid),
            buf(rows, hid),
            buf(hid, rows),
            buf(blocks, 2, 2, ranks // 4, R, share),
            buf(blocks, 2, ranks // 4, R, share),
            buf(blocks, 2, R, share // 2),
            buf(blocks, 2, R, share // 2),
            buf(blocks, R, share // 2),
            buf(blocks, R, share // 2),
            buf(rows, share),
            buf(rows, share),
            buf(pieces, tok, strip),
            buf(width, hid),
            buf(width, hid),
            buf(hid, width),
            buf(*token_values.shape),
            buf(*write_keys.shape),
            buf(*read_keys.shape),
            buf(*log_decay.shape, dtype=F32),
            buf(*out_gate.shape),
            buf(*out_proj.shape),
            buf(tok, inner, dtype=F32),
            buf(tok, inner, dtype=F32),
            buf(tok, inner, dtype=F32),
            buf(heads, tok, tok, dtype=F32),
            buf(heads, tok, tok),
            buf(tok, inner),
            buf(n, inner, STATE),
            buf(n, max(heads, 8), STATE, dtype=F32),
            buf(n, inner, STATE),
            buf(inner, STATE),
            buf(n * tok if far else tok, inner),
            buf((n - 1) * tok if far else 16, strip if far else 128),
            buf(tok, inner, dtype=F32),
            buf(tok, inner),
            buf(tok, inner),
            buf(*write_keys.shape, dtype=F32),
            buf(tok, inner),
            buf(*write_keys.shape),
            buf(*read_keys.shape),
            buf(tok, inner),
            buf(*((strip, inner) if far else (8, 128)), dtype=F32),
            pltpu.SemaphoreType.DMA((slots,)),
            pltpu.SemaphoreType.DMA((slots,)),
            pltpu.SemaphoreType.DMA((24 + pieces,)),
        ],
        compiler_params=pltpu.CompilerParams(
            collective_id=1, has_side_effects=True, vmem_limit_bytes=60 * 1024 * 1024
        ),
    )(*operands)
    value_grad, write_grad, read_grad, gate_grad = got[:4]
    grad_gate, grad_up, grad_down = got[-3:]
    if far:
        proj_grad = got[4]
    else:
        proj_part = dot(got[4], got[5], 0, 0).astype(BF16)
        proj_grad = lax.psum_scatter(proj_part, "sp", scatter_dimension=0, tiled=True).astype(F32)
    return (
        value_grad,
        write_grad,
        read_grad,
        gate_grad,
        proj_grad,
        grad_gate[None],
        grad_up[None],
        grad_down[None],
    )


def solution(mesh):
    return jax.shard_map(
        body,
        mesh=mesh,
        in_specs=(
            P("sp", "tp"),
            P("sp", "tp"),
            P("sp", "tp"),
            P("tp", "sp"),
            P("sp", "tp"),
            P(None, "tp"),
            P("sp", None),
            P("sp", None),
            P("sp", None),
            P("sp", None),
            P("sp", None, "tp"),
            P("sp", None, "tp"),
            P("sp", "tp", None),
        ),
        out_specs=(
            P("sp", "tp"),
            P("sp", "tp"),
            P("sp", "tp"),
            P("sp", "tp"),
            P("sp", "tp"),
            P("sp", None, "tp"),
            P("sp", None, "tp"),
            P("sp", "tp", None),
        ),
        check_vma=False,
    )
```

```python
import functools

import jax
import jax.numpy as jnp
from jax import lax
from jax.experimental import pallas as pl
from jax.experimental.pallas import tpu as pltpu
from jax.sharding import PartitionSpec as P

HEAD_DIM = 64
STATE = 128

F32 = jnp.float32
BF16 = jnp.bfloat16
MESH = pl.DeviceIdType.MESH
VMEM_LIMIT = 54 * 1024 * 1024


def dot(a, b, ca=1, cb=0):
    return lax.dot_general(a, b, (((ca,), (cb,)), ((), ())), preferred_element_type=F32)


class Links:
    def __init__(self, send_sem, recv_sem):
        self.send_sem, self.recv_sem = send_sem, recv_sem
        self.used = 0
        self.started = []

    def slot(self):
        self.used += 1
        return self.used - 1

    def copy(self, slot, src, dst, device):
        return pltpu.make_async_remote_copy(
            src_ref=src,
            dst_ref=dst,
            send_sem=self.send_sem.at[slot],
            recv_sem=self.recv_sem.at[slot],
            device_id=device,
            device_id_type=MESH,
        )

    def start(self, slot, src, dst, device):
        made = self.copy(slot, src, dst, device)
        made.start()
        self.started.append(made)

    def arrived(self, slot, dst, device):
        self.copy(slot, dst, dst, device).wait_recv()

    def finish(self):
        for made in self.started:
            made.wait_send()


class Spread:
    def __init__(self, links, t, window):
        self.links, self.window = links, window
        self.other, self.across, self.along = ({"tp": t ^ bit} for bit in (1, 2, 4))
        self.slots = [links.slot() for _ in range(9)]

    def send(self, kind, bits, part, device):
        w = self.window(bits, part)
        self.links.start(self.slots[kind], w, w, device)

    def got(self, kind, bits, part, device):
        self.links.arrived(self.slots[kind], self.window(bits, part), device)

    def p0(self):
        self.send(1, 0, None, self.across)
        self.send(2, 0, None, self.along)
        self.send(5, 0, None, self.other)

    def p1(self):
        self.got(1, 2, None, self.across)
        self.send(3, 2, 0, self.along)
        self.send(6, 2, None, self.other)
        self.got(2, 4, None, self.along)
        self.send(4, 4, 1, self.across)
        self.send(7, 4, None, self.other)

    def p2(self):
        self.got(3, 6, 0, self.along)
        self.got(4, 6, 1, self.across)
        self.send(8, 6, None, self.other)

    def p3(self):
        for kind, bits in ((5, 1), (6, 3), (7, 5), (8, 7)):
            self.got(kind, bits, None, self.other)


def greet(n, t, s):
    peers = [{"tp": t ^ bit} for bit in (1, 2, 4)] + [{"sp": s ^ k} for k in range(1, n)]
    barrier = pltpu.get_barrier_semaphore()
    for peer in peers:
        pl.semaphore_signal(barrier, inc=1, device_id=peer, device_id_type=MESH)
    pl.semaphore_wait(barrier, len(peers))


def main_kernel(
    n,
    ranks,
    pieces,
    ids_in,
    weights_in,
    mixed,
    cotangent,
    w_gate,
    w_up,
    w_down,
    values_in,
    writes_in,
    reads_in,
    decay_in,
    gate_in,
    proj_in,
    DV,
    DWK,
    DRK,
    DGT,
    GW,
    UW,
    DW,
    *refs,
):
    outs_proj = refs[: 1 if pieces == n else 2]
    (
        IDS, RW, M, C, W2, WD, X, S, SX, SS, ONE, WCOL, DGU, HID, HT,
        PB, RB, RX, RY, RX2, RY2, FIN, CB, G,
        TV, WK, RK, LD, OGT, OP, LW, TW, Y, DEC, KT, TLD, END, TOT, BK, ENT, GB, F,
        OG, OB, LED, DWF, MP, CP, ACT, DFAC, BACK,
        send_sem, recv_sem, local_sem,
    ) = refs[len(outs_proj) :]
    PJ = outs_proj[0]
    t = lax.axis_index("tp")
    s = lax.axis_index("sp")
    tok, width = M.shape
    hid = WD.shape[0]
    cap = CB.shape[0] // n
    share = width // ranks
    half_share = share // 2
    blocks = PB.shape[0]
    group = n // blocks
    R = group * cap
    strip = width // pieces
    pw = strip // ranks
    heads = LD.shape[0]
    groups = WK.shape[1] // STATE
    per_group = heads // groups
    chan = per_group * HEAD_DIM
    c = lax.rem(t, 2)
    mx = lax.rem(t // 2, 2)
    my = t // 4
    links = Links(send_sem, recv_sem)
    other, across, along = ({"tp": t ^ bit} for bit in (1, 2, 4))
    loaded = [0]

    def load(src, dst):
        made = pltpu.make_async_copy(src, dst, local_sem.at[loaded[0]])
        loaded[0] += 1
        made.start()
        return made

    mine = pl.ds(pl.multiple_of(t * share, 128), share)
    first_loads = [
        load(ids_in, IDS),
        load(weights_in, RW),
        load(mixed.at[:, mine], MP),
        load(cotangent.at[:, mine], CP),
    ]
    row_loads = [load(mixed, M), load(cotangent, C)]
    mix_loads = [
        load(decay_in, LD),
        load(writes_in, WK),
        load(values_in, TV),
        load(reads_in, RK),
        load(gate_in, OGT),
    ]
    expert_loads = [
        load(w_gate, W2.at[:, pl.ds(0, hid)]),
        load(w_up, W2.at[:, pl.ds(hid, hid)]),
        load(w_down, WD),
    ]
    proj_load = load(proj_in, OP)
    greet(n, t, s)
    for made in first_loads:
        made.wait()

    rows_n = max(n, 8)
    lane = lax.broadcasted_iota(jnp.int32, (rows_n, tok), 0) ^ s
    names = [IDS[i : i + 1, :] == lane for i in range(IDS.shape[0])]
    member = functools.reduce(jnp.logical_or, names)
    weight = sum(jnp.where(names[i], RW[i : i + 1, :], 0.0) for i in range(IDS.shape[0]))
    row_of = lax.broadcasted_iota(jnp.int32, (tok, tok), 0)
    col_of = lax.broadcasted_iota(jnp.int32, (tok, tok), 1)
    earlier = (row_of < col_of).astype(F32).astype(BF16)
    slot = dot(member.astype(F32).astype(BF16), earlier)
    slot = jnp.where(member, slot, -1.0).astype(jnp.int32)
    place = lax.broadcasted_iota(jnp.int32, (cap, tok), 0)

    z_slots = [[links.slot() for _ in range(n)] for _ in range(2)]
    m_part, c_part = MP[...], CP[...]
    for k in list(range(1, n)) + [0]:
        rows = pl.ds(k * cap, cap)
        chosen = slot[k : k + 1, :] == place
        pick = chosen.astype(F32).astype(BF16)
        row_weight = jnp.sum(jnp.where(chosen, weight[k : k + 1, :], 0.0), axis=1, keepdims=True)
        ONE[rows, :] = pick
        if k:
            SX[k - 1] = dot(pick, m_part).astype(BF16)
            SS[k - 1] = (dot(pick, c_part) * row_weight).astype(BF16)
            for a, (src, dst) in enumerate(((SX, X), (SS, S))):
                links.start(z_slots[a][k], src.at[k - 1], dst.at[rows, mine], {"sp": s ^ k})
        else:
            WCOL[...] = jnp.broadcast_to(row_weight, WCOL.shape)

    def local_rows():
        for made in row_loads:
            made.wait()

        def some(i, _):
            at = pl.ds(pl.multiple_of(i * share, 128), share)
            pick = ONE[pl.ds(0, cap), :]
            X[pl.ds(0, cap), at] = dot(pick, M[:, at]).astype(BF16)
            S[pl.ds(0, cap), at] = (dot(pick, C[:, at]) * WCOL[:, :1]).astype(BF16)
            return 0

        lax.fori_loop(0, ranks, some, 0)

    chunks = {}
    for q in range(blocks):
        first = cap if q == 0 else 0
        if first == R:
            continue
        for a, ref in enumerate((X, S)):

            def window(bits, part, ref=ref, row=q * R + first, count=R - first):
                begin, size = (t ^ bits) * share, share
                if part is not None:
                    begin, size = begin + part * half_share, half_share
                return ref.at[pl.ds(row, count), pl.ds(pl.multiple_of(begin, 128), size)]

            chunks[(q, a)] = Spread(links, t, window)

    def p0(q, a):
        ref = (X, S)[a]
        for k in range(q * group, (q + 1) * group):
            if k:
                links.arrived(z_slots[a][k], ref.at[pl.ds(k * cap, cap), mine], {"sp": s ^ k})
        chunks[(q, a)].p0()

    def expert_a(q):
        r = pl.ds(q * R, R)
        both = dot(X[r, :], W2[...])
        gate, up = both[:, :hid], both[:, hid:]
        sigma = jax.nn.sigmoid(gate)
        act = gate * sigma
        HID[r, :] = (act * up).astype(BF16)
        ACT[...] = act
        DFAC[...] = up * sigma * (1.0 + gate * (1.0 - sigma))

    def expert_b(q):
        r = pl.ds(q * R, R)
        d_act = dot(S[r, :], WD[...], 1, 1)
        DGU[r, pl.ds(0, hid)] = (d_act * DFAC[...]).astype(BF16)
        DGU[r, pl.ds(hid, hid)] = (d_act * ACT[...]).astype(BF16)

    def portion(q):
        r = pl.ds(q * R, R)
        step = 256
        for j in range(pieces):

            def some(i, _, j=j):
                begin = pl.multiple_of(j * strip + i * step, 128)
                tile = dot(DGU[r, :], W2[pl.ds(begin, step), :], 1, 1).astype(BF16)
                if pw >= step:
                    per = pw // step
                    dest, off = i // per, lax.rem(i, per) * step
                    at = pl.ds(pl.multiple_of(j * pw + off, 128), step)
                    PB[q, lax.rem(dest, 2), dest // 4, lax.rem(dest // 2, 2), :, at] = tile
                else:
                    at = pl.ds(j * pw, pw)
                    PB[q, 0, i // 2, lax.rem(i, 2), :, at] = tile[:, :pw]
                    PB[q, 1, i // 2, lax.rem(i, 2), :, at] = tile[:, pw:]
                return 0

            lax.fori_loop(0, strip // step, some, 0)

    rs_slots = [[links.slot() for _ in range(5)] for _ in range(blocks)]
    back_slots = [links.slot() for _ in range(n)]
    lo, hi = pl.ds(0, half_share), pl.ds(half_share, half_share)

    def r0(q):
        links.start(rs_slots[q][0], PB.at[q, 1 - c], RB.at[q], other)

    def r1(q):
        links.arrived(rs_slots[q][0], RB.at[q], other)

        def add(i, _):
            a, b = i // 2, lax.rem(i, 2)
            RB[q, a, b] = (PB[q, c, a, b].astype(F32) + RB[q, a, b].astype(F32)).astype(BF16)
            return 0

        lax.fori_loop(0, ranks // 2, add, 0)
        links.start(rs_slots[q][1], RB.at[q, :, 1 - mx, :, lo], RX.at[q], across)
        links.start(rs_slots[q][2], RB.at[q, 1 - my, :, :, hi], RY.at[q], along)

    def r2(q):
        links.arrived(rs_slots[q][1], RX.at[q], across)
        for i in range(2):
            RX[q, i] = (RB[q, i, mx, :, lo].astype(F32) + RX[q, i].astype(F32)).astype(BF16)
        links.start(rs_slots[q][3], RX.at[q, 1 - my], RX2.at[q], along)
        links.arrived(rs_slots[q][2], RY.at[q], along)
        for i in range(2):
            RY[q, i] = (RB[q, my, i, :, hi].astype(F32) + RY[q, i].astype(F32)).astype(BF16)
        links.start(rs_slots[q][4], RY.at[q, 1 - mx], RY2.at[q], across)

    def r3(q):
        r = pl.ds(q * R, R)
        links.arrived(rs_slots[q][3], RX2.at[q], along)
        FIN[r, lo] = (RX[q, my].astype(F32) + RX2[q].astype(F32)).astype(BF16)
        links.arrived(rs_slots[q][4], RY2.at[q], across)
        FIN[r, hi] = (RY[q, mx].astype(F32) + RY2[q].astype(F32)).astype(BF16)
        for k in range(q * group, (q + 1) * group):
            rows = pl.ds(k * cap, cap)
            if k:
                links.start(back_slots[k], FIN.at[rows, :], CB.at[rows, :], {"sp": s ^ k})
            else:
                CB[rows, :] = FIN[rows, :]

    def grads_gate_up(first, last):
        def some(i, _):
            at = pl.ds(pl.multiple_of(i * 256, 128), 256)
            tile = dot(X[:, at], DGU[...], 0, 0).astype(BF16)
            GW[at, :] = tile[:, :hid]
            UW[at, :] = tile[:, hid:]
            return 0

        lax.fori_loop(first, last, some, 0)

    def grads_down():
        HT[...] = HID[...].T

        def some(i, _):
            at = pl.ds(pl.multiple_of(i * 512, 128), 512)
            DW[:, at] = dot(HT[...], S[:, at]).astype(BF16)
            return 0

        lax.fori_loop(0, width // 512, some, 0)

    head_of = lax.broadcasted_iota(jnp.int32, (tok, chan), 1) // HEAD_DIM
    end_slots = [[links.slot() for _ in range(n)] for _ in range(2)]
    gated_slots = [links.slot() for _ in range(n)]
    state_slots = [links.slot() for _ in range(n)]

    def keys(ref, g):
        return ref[:, g * STATE : (g + 1) * STATE]

    def wide(columns):
        return jnp.concatenate(
            [jnp.broadcast_to(columns[:, h : h + 1], (tok, HEAD_DIM)) for h in range(heads)], axis=1
        )

    def everyone(slots, src, dst):
        for k in range(1, n):
            links.start(slots[k], src, dst(k), {"sp": s ^ k})

    def mixer_ends():
        for made in mix_loads:
            made.wait()
        pad = max(heads, 8) - heads
        decays = LD[...]
        if pad:
            decays = jnp.concatenate([decays, jnp.zeros((pad, tok), F32)], axis=0)
        upto = (row_of <= col_of).astype(F32)
        cumul = lax.dot_general(
            decays,
            upto,
            (((1,), (0,)), ((), ())),
            precision=lax.Precision.HIGHEST,
            preferred_element_type=F32,
        )
        total = cumul[:, tok - 1 :]
        TOT[s] = jnp.broadcast_to(total, TOT.shape[1:])
        columns = cumul.T
        spread = wide(columns)
        LW[...] = jnp.exp(spread)
        tails = jnp.exp(spread[tok - 1 :, :] - spread)
        TW[...] = tails
        TLD[...] = (TV[...].astype(F32) * tails).astype(BF16)
        for g in range(groups):
            at = pl.ds(g * chan, chan)
            END[s, at, :] = dot(TLD[:, at], keys(WK, g), 0, 0).astype(BF16)
        everyone(end_slots[0], END.at[s], lambda k: END.at[s])
        everyone(end_slots[1], TOT.at[s], lambda k: TOT.at[s])
        for h in range(heads):
            span = columns[:, h : h + 1] - cumul[h : h + 1, :]
            DEC[h] = jnp.exp(jnp.where(row_of >= col_of, span, -jnp.inf))

    def mixer_inner():
        for g in range(groups):
            scores = dot(keys(RK, g), keys(WK, g), 1, 1)
            at = pl.ds(g * chan, chan)
            inner = jnp.zeros((tok, chan), F32)
            for r in range(per_group):
                h = g * per_group + r
                kept = scores * DEC[h]
                KT[h] = kept.T.astype(BF16)
                inner = jnp.where(head_of == r, dot(kept.astype(BF16), TV[:, at]), inner)
            Y[:, at] = inner

    def factor(j):
        return jnp.concatenate(
            [jnp.broadcast_to(jnp.exp(TOT[j][h : h + 1, :]), (HEAD_DIM, STATE)) for h in range(heads)],
            axis=0,
        )

    def mixer_gated():
        for k in range(1, n):
            links.arrived(end_slots[0][k], END.at[s ^ k], {"sp": s ^ k})
            links.arrived(end_slots[1][k], TOT.at[s ^ k], {"sp": s ^ k})
        state = jnp.zeros(END.shape[1:], F32)
        for j in range(n - 1):
            state = jnp.where(j < s, factor(j) * state + END[j].astype(F32), state)
        ENT[...] = state.astype(BF16)
        for g in range(groups):
            at = pl.ds(g * chan, chan)
            carried = dot(keys(RK, g), ENT[at, :], 1, 1)
            y = Y[:, at] + carried * LW[:, at]
            Y[:, at] = y
            gate = OGT[:, at].astype(F32)
            GB[pl.ds(0, tok), at] = (y * (gate * jax.nn.sigmoid(gate))).astype(BF16)
        if pieces == n:
            own = GB.at[pl.ds(0, tok), :]
            everyone(gated_slots, own, lambda k: GB.at[pl.ds(k * tok, tok), :])

    def mixer_states():
        for g in range(groups):
            at = pl.ds(g * chan, chan)
            gate = OGT[:, at].astype(F32)
            sig = jax.nn.sigmoid(gate)
            outer = OG[:, at] * (gate * sig)
            OB[:, at] = outer.astype(BF16)
            LED[:, at] = (outer * LW[:, at]).astype(BF16)
            BK[s, at, :] = dot(LED[:, at], keys(RK, g), 0, 0).astype(BF16)
        everyone(state_slots, BK.at[s], lambda k: BK.at[s])

    def mixer_scores():
        for g in range(groups):
            at = pl.ds(g * chan, chan)
            gate = OGT[:, at].astype(F32)
            sig = jax.nn.sigmoid(gate)
            DGT[:, at] = (OG[:, at] * Y[:, at] * sig * (1.0 + gate * (1.0 - sig))).astype(BF16)
            d_scores = jnp.zeros((tok, tok), F32)
            d_values = jnp.zeros((tok, chan), F32)
            for r in range(per_group):
                h = g * per_group + r
                one = jnp.where(head_of == r, OB[:, at].astype(F32), 0.0).astype(BF16)
                d_scores = d_scores + dot(one, TV[:, at], 1, 1) * DEC[h]
                d_values = jnp.where(head_of == r, dot(KT[h], OB[:, at]), d_values)
            OG[:, at] = d_values
            d_scores = d_scores.astype(BF16)
            ks = pl.ds(g * STATE, STATE)
            DRK[:, ks] = (dot(d_scores, keys(WK, g)) + dot(LED[:, at], ENT[at, :])).astype(BF16)
            DWF[:, ks] = dot(d_scores, keys(RK, g), 0, 0)

    def mixer_last():
        for k in range(1, n):
            links.arrived(state_slots[k], BK.at[s ^ k], {"sp": s ^ k})
        state = jnp.zeros(BK.shape[1:], F32)
        for j in range(n - 1, 0, -1):
            state = jnp.where(j > s, factor(j) * state + BK[j].astype(F32), state)
        leaving = state.astype(BF16)
        for g in range(groups):
            at = pl.ds(g * chan, chan)
            ks = pl.ds(g * STATE, STATE)
            mine_of = leaving[g * chan : (g + 1) * chan]
            DWK[:, ks] = (DWF[:, ks] + dot(TLD[:, at], mine_of)).astype(BF16)
            d_values = OG[:, at] + dot(keys(WK, g), mine_of, 1, 1) * TW[:, at]
            DV[:, at] = d_values.astype(BF16)

    order = [key for key in chunks]
    count = len(order)

    def forward(i):
        if i < count:
            p0(*order[i])
        if 0 <= i - 1 < count:
            chunks[order[i - 1]].p1()
        if 0 <= i - 2 < count:
            chunks[order[i - 2]].p2()

    def landed(q, a):
        if (q, a) in chunks:
            chunks[(q, a)].p3()

    def rest(q):
        landed(q, 1)
        expert_b(q)
        portion(q)
        r0(q)

    def add_back(first, last, start):
        rows = pl.ds(first * cap, (last - first) * cap)
        for k in range(max(first, 1), last):
            one = pl.ds(k * cap, cap)
            links.arrived(back_slots[k], CB.at[one, :], {"sp": s ^ k})
        part = dot(ONE[rows, :], CB[rows, :], 0, 0)
        BACK[...] = part if start else BACK[...] + part

    tiles = width // 256
    mixer_ends()
    if blocks == 4 and (0, 0) not in chunks:
        forward(0)
        local_rows()
        for made in expert_loads:
            made.wait()
        forward(1)
        expert_a(0)
        expert_b(0)
        forward(2)
        portion(0)
        r0(0)
        forward(3)
        mixer_inner()
        landed(1, 0)
        expert_a(1)
        forward(4)
        rest(1)
        forward(5)
        r1(1)
        mixer_gated()
        landed(2, 0)
        expert_a(2)
        forward(6)
        rest(2)
        forward(7)
        r2(1)
        r1(2)
        landed(3, 0)
        expert_a(3)
        r3(1)
        rest(3)
        r2(2)
        r1(3)
        r1(0)
        grads_gate_up(0, tiles // 8)
        r3(2)
        r2(3)
        grads_gate_up(tiles // 8, tiles // 4)
        r2(0)
        r3(3)
        grads_gate_up(tiles // 4, tiles // 2)
        add_back(1, 3, True)
        r3(0)
        add_back(0, 1, False)
        add_back(3, 4, False)
    else:
        local_rows()
        for made in expert_loads:
            made.wait()
        mixer_inner()
        mixer_gated()
        for i in range(count + 2):
            forward(i)
        for q in range(blocks):
            landed(q, 0)
            expert_a(q)
            rest(q)
        for stage in (r1, r2, r3):
            for q in range(blocks):
                stage(q)
        grads_gate_up(0, tiles // 2)
        add_back(0, n, True)

    half_tok = tok // 2
    cuts = 4
    cut = tok // cuts
    gathers = []
    for i in range(cuts):

        def window(bits, part, i=i):
            row, rows = i * cut, cut
            if part is not None:
                row, rows = row + part * (cut // 2), cut // 2
            return G.at[:, pl.ds(row, rows), pl.ds(pl.multiple_of((t ^ bits) * pw, 128), pw)]

        gathers.append(Spread(links, t, window))
    here = pl.ds(pl.multiple_of(t * pw, 128), pw)
    for i in range(cuts):
        rows = pl.ds(i * cut, cut)
        for j in range(pieces):
            cot = C[rows, pl.ds(pl.multiple_of(j * strip + t * pw, 128), pw)].astype(F32)
            G[j, rows, here] = (cot + BACK[rows, pl.ds(j * pw, pw)]).astype(BF16)
        gathers[i].p0()

    fars = []
    if pieces == n:
        far_slots = [links.slot() for _ in range(n)]
        for k in range(1, n):
            rows = pl.ds((k - 1) * tok, tok)
            links.start(far_slots[k], G.at[s ^ k, :, here], F.at[rows, here], {"sp": s ^ k})

            def window(bits, part, k=k):
                row, rows = (k - 1) * tok, tok
                if part is not None:
                    row, rows = row + part * half_tok, half_tok
                return F.at[pl.ds(row, rows), pl.ds(pl.multiple_of((t ^ bits) * pw, 128), pw)]

            fars.append(Spread(links, t, window))

    def far_p0(k):
        rows = pl.ds((k - 1) * tok, tok)
        links.arrived(far_slots[k], F.at[rows, here], {"sp": s ^ k})
        fars[k - 1].p0()

    grads_down()
    for i in range(cuts):
        gathers[i].p1()
        if i:
            gathers[i - 1].p2()
    gathers[cuts - 1].p2()
    for k in range(1, len(fars) + 1):
        far_p0(k)
    for i in range(cuts):
        gathers[i].p3()
    proj_load.wait()
    OG[...] = sum(dot(G[j], OP[pl.ds(j * strip, strip), :]) for j in range(pieces))
    def proj_own(i, _):
        at = pl.ds(pl.multiple_of(i * 256, 128), 256)
        PJ[at, :] = dot(G[s, :, at], GB[pl.ds(0, tok), :], 0, 0)
        return 0

    def proj_far(i, _):
        at = pl.ds(pl.multiple_of(i * 256, 128), 256)
        PJ[at, :] += dot(F[:, at], GB[pl.ds(tok, (n - 1) * tok), :], 0, 0)
        return 0

    mixer_states()
    for far in fars:
        far.p1()
    mixer_scores()
    for far in fars:
        far.p2()
    if pieces == n:
        lax.fori_loop(0, strip // 256, proj_own, 0)
    grads_gate_up(tiles // 2, tiles)
    mixer_last()
    if pieces == n:
        for far in fars:
            far.p3()
        for k in range(1, n):
            links.arrived(gated_slots[k], GB.at[pl.ds(k * tok, tok), :], {"sp": s ^ k})
        lax.fori_loop(0, strip // 256, proj_far, 0)
    else:
        for j in range(pieces):
            outs_proj[0][:, pl.ds(j * strip, strip)] = G[j]
        outs_proj[1][...] = GB[pl.ds(0, tok), :]
    links.finish()


def place_kernel(count, *refs):
    sources, places, sem = refs[:count], refs[count : 2 * count], refs[-1]
    made = [pltpu.make_async_copy(sources[i], places[i], sem.at[i]) for i in range(count)]
    for one in made:
        one.start()
    for one in made:
        one.wait()


def place(arrays):
    any_ = pl.BlockSpec(memory_space=pl.ANY)
    count = len(arrays)
    return pl.pallas_call(
        functools.partial(place_kernel, count),
        out_shape=[jax.ShapeDtypeStruct(a.shape, a.dtype) for a in arrays],
        in_specs=[any_] * count,
        out_specs=[any_] * count,
        scratch_shapes=[pltpu.SemaphoreType.DMA((count,))],
        compiler_params=pltpu.CompilerParams(vmem_limit_bytes=1024 * 1024),
    )(*arrays)


def body(
    token_values,
    write_keys,
    read_keys,
    log_decay,
    out_gate,
    out_proj,
    mixed,
    cotangent,
    route_ids,
    route_weights,
    w_gate,
    w_up,
    w_down,
):
    tok, width = mixed.shape
    n = lax.axis_size("sp")
    ranks = lax.axis_size("tp")
    hid = w_gate.shape[2]
    inner = token_values.shape[1]
    heads = log_decay.shape[0]
    share = width // ranks
    cap = 3 * tok // n
    rows = n * cap
    pieces = n if (width // n // ranks) % 128 == 0 else 1
    far = pieces == n
    strip = width // pieces
    blocks = 4 if n % 4 == 0 else n
    R = rows // blocks
    slots = 2 * n + 2 * blocks * 9 + 5 * blocks + 6 * n + 18 + 9 * n
    any_ = pl.BlockSpec(memory_space=pl.ANY)

    def buf(*shape, dtype=BF16):
        return pltpu.VMEM(shape, dtype)

    def like(a):
        return pltpu.VMEM(a.shape, a.dtype)

    if far:
        proj_shapes = [pltpu.VMEM((strip, inner), F32)]
    else:
        proj_shapes = [pltpu.VMEM((tok, width), BF16), pltpu.VMEM((tok, inner), BF16)]
    operands = [
        route_ids.T,
        route_weights.T,
        mixed,
        cotangent,
        w_gate[0],
        w_up[0],
        w_down[0],
        token_values,
        write_keys,
        read_keys,
        log_decay,
        out_gate,
        out_proj,
    ]
    outputs = (
        [like(token_values), like(write_keys), like(read_keys), like(out_gate)]
        + [like(w_gate[0]), like(w_up[0]), like(w_down[0])]
        + proj_shapes
    )
    got = pl.pallas_call(
        functools.partial(main_kernel, n, ranks, pieces),
        out_shape=outputs,
        in_specs=[any_] * len(operands),
        out_specs=[pl.BlockSpec(memory_space=pltpu.VMEM)] * len(outputs),
        scratch_shapes=[
            buf(*route_ids.T.shape, dtype=jnp.int32),
            buf(*route_ids.T.shape, dtype=F32),
            buf(tok, width),
            buf(tok, width),
            buf(width, 2 * hid),
            buf(hid, width),
            buf(rows, width),
            buf(rows, width),
            buf(n - 1, cap, share),
            buf(n - 1, cap, share),
            buf(rows, tok),
            buf(cap, 128, dtype=F32),
            buf(rows, 2 * hid),
            buf(rows, hid),
            buf(hid, rows),
            buf(blocks, 2, 2, ranks // 4, R, share),
            buf(blocks, 2, ranks // 4, R, share),
            buf(blocks, 2, R, share // 2),
            buf(blocks, 2, R, share // 2),
            buf(blocks, R, share // 2),
            buf(blocks, R, share // 2),
            buf(rows, share),
            buf(rows, share),
            buf(pieces, tok, strip),
            buf(*token_values.shape),
            buf(*write_keys.shape),
            buf(*read_keys.shape),
            buf(*log_decay.shape, dtype=F32),
            buf(*out_gate.shape),
            buf(*out_proj.shape),
            buf(tok, inner, dtype=F32),
            buf(tok, inner, dtype=F32),
            buf(tok, inner, dtype=F32),
            buf(heads, tok, tok, dtype=F32),
            buf(heads, tok, tok),
            buf(tok, inner),
            buf(n, inner, STATE),
            buf(n, max(heads, 8), STATE, dtype=F32),
            buf(n, inner, STATE),
            buf(inner, STATE),
            buf(n * tok if far else tok, inner),
            buf((n - 1) * tok if far else 16, strip if far else 128),
            buf(tok, inner, dtype=F32),
            buf(tok, inner),
            buf(tok, inner),
            buf(*write_keys.shape, dtype=F32),
            buf(tok, share),
            buf(tok, share),
            buf(R, hid, dtype=F32),
            buf(R, hid, dtype=F32),
            buf(tok, share, dtype=F32),
            pltpu.SemaphoreType.DMA((slots,)),
            pltpu.SemaphoreType.DMA((slots,)),
            pltpu.SemaphoreType.DMA((24 + pieces,)),
        ],
        compiler_params=pltpu.CompilerParams(
            collective_id=1, has_side_effects=True, vmem_limit_bytes=VMEM_LIMIT
        ),
    )(*operands)
    placed = place(got if far else got[:7])
    value_grad, write_grad, read_grad, gate_grad, grad_gate, grad_up, grad_down = placed[:7]
    if far:
        proj_grad = placed[7]
    else:
        proj_part = dot(got[7], got[8], 0, 0).astype(BF16)
        proj_grad = lax.psum_scatter(proj_part, "sp", scatter_dimension=0, tiled=True).astype(F32)
    return (
        value_grad,
        write_grad,
        read_grad,
        gate_grad,
        proj_grad,
        grad_gate[None],
        grad_up[None],
        grad_down[None],
    )


def solution(mesh):
    return jax.shard_map(
        body,
        mesh=mesh,
        in_specs=(
            P("sp", "tp"),
            P("sp", "tp"),
            P("sp", "tp"),
            P("tp", "sp"),
            P("sp", "tp"),
            P(None, "tp"),
            P("sp", None),
            P("sp", None),
            P("sp", None),
            P("sp", None),
            P("sp", None, "tp"),
            P("sp", None, "tp"),
            P("sp", "tp", None),
        ),
        out_specs=(
            P("sp", "tp"),
            P("sp", "tp"),
            P("sp", "tp"),
            P("sp", "tp"),
            P("sp", "tp"),
            P("sp", None, "tp"),
            P("sp", None, "tp"),
            P("sp", "tp", None),
        ),
        check_vma=False,
    )
```

```python
import functools

import jax
import jax.numpy as jnp
from jax import lax
from jax.experimental import pallas as pl
from jax.experimental.pallas import tpu as pltpu
from jax.sharding import PartitionSpec as P

HEAD_DIM = 64
STATE = 128

F32 = jnp.float32
BF16 = jnp.bfloat16
MESH = pl.DeviceIdType.MESH
VMEM_LIMIT = 54 * 1024 * 1024


def dot(a, b, ca=1, cb=0):
    return lax.dot_general(a, b, (((ca,), (cb,)), ((), ())), preferred_element_type=F32)


class Links:
    def __init__(self, send_sem, recv_sem):
        self.send_sem, self.recv_sem = send_sem, recv_sem
        self.used = 0
        self.started = []

    def slot(self):
        self.used += 1
        return self.used - 1

    def copy(self, slot, src, dst, device):
        return pltpu.make_async_remote_copy(
            src_ref=src,
            dst_ref=dst,
            send_sem=self.send_sem.at[slot],
            recv_sem=self.recv_sem.at[slot],
            device_id=device,
            device_id_type=MESH,
        )

    def start(self, slot, src, dst, device):
        made = self.copy(slot, src, dst, device)
        made.start()
        self.started.append(made)

    def arrived(self, slot, dst, device):
        self.copy(slot, dst, dst, device).wait_recv()

    def finish(self):
        for made in self.started:
            made.wait_send()


class Spread:
    def __init__(self, links, t, window):
        self.links, self.window = links, window
        self.other, self.across, self.along = ({"tp": t ^ bit} for bit in (1, 2, 4))
        self.slots = [links.slot() for _ in range(9)]

    def send(self, kind, bits, part, device):
        w = self.window(bits, part)
        self.links.start(self.slots[kind], w, w, device)

    def got(self, kind, bits, part, device):
        self.links.arrived(self.slots[kind], self.window(bits, part), device)

    def p0(self):
        self.send(1, 0, None, self.across)
        self.send(2, 0, None, self.along)
        self.send(5, 0, None, self.other)

    def p1(self):
        self.got(1, 2, None, self.across)
        self.send(3, 2, 0, self.along)
        self.send(6, 2, None, self.other)
        self.got(2, 4, None, self.along)
        self.send(4, 4, 1, self.across)
        self.send(7, 4, None, self.other)

    def p2(self):
        self.got(3, 6, 0, self.along)
        self.got(4, 6, 1, self.across)
        self.send(8, 6, None, self.other)

    def p3(self):
        for kind, bits in ((5, 1), (6, 3), (7, 5), (8, 7)):
            self.got(kind, bits, None, self.other)


def greet(n, t, s):
    peers = [{"tp": t ^ bit} for bit in (1, 2, 4)] + [{"sp": s ^ k} for k in range(1, n)]
    barrier = pltpu.get_barrier_semaphore()
    for peer in peers:
        pl.semaphore_signal(barrier, inc=1, device_id=peer, device_id_type=MESH)
    pl.semaphore_wait(barrier, len(peers))


def main_kernel(
    n,
    ranks,
    pieces,
    ids_in,
    weights_in,
    mixed,
    cotangent,
    w_gate,
    w_up,
    w_down,
    values_in,
    writes_in,
    reads_in,
    decay_in,
    gate_in,
    proj_in,
    DV,
    DWK,
    DRK,
    DGT,
    GW,
    UW,
    DW,
    *refs,
):
    outs_proj = refs[: 1 if pieces == n else 2]
    (
        IDS, RW, M, C, W2, WD, X, S, SX, SS, ONE, WCOL, DGU, HID, HT,
        PB, RB, RX, RY, RX2, RY2, FIN, CB, G,
        TV, WK, RK, LD, OGT, OP, LW, TW, Y, DEC, KT, TLD, END, TOT, BK, ENT, GB, F,
        OG, OB, LED, DWF, MP, CP, ACT, DFAC, BACK,
        send_sem, recv_sem, local_sem,
    ) = refs[len(outs_proj) :]
    PJ = outs_proj[0]
    t = lax.axis_index("tp")
    s = lax.axis_index("sp")
    tok, width = M.shape
    hid = WD.shape[0]
    cap = CB.shape[0] // n
    share = width // ranks
    half_share = share // 2
    blocks = PB.shape[0]
    group = n // blocks
    R = group * cap
    strip = width // pieces
    pw = strip // ranks
    heads = LD.shape[0]
    groups = WK.shape[1] // STATE
    per_group = heads // groups
    chan = per_group * HEAD_DIM
    c = lax.rem(t, 2)
    mx = lax.rem(t // 2, 2)
    my = t // 4
    links = Links(send_sem, recv_sem)
    other, across, along = ({"tp": t ^ bit} for bit in (1, 2, 4))
    loaded = [0]

    def load(src, dst):
        made = pltpu.make_async_copy(src, dst, local_sem.at[loaded[0]])
        loaded[0] += 1
        made.start()
        return made

    mine = pl.ds(pl.multiple_of(t * share, 128), share)
    first_loads = [
        load(ids_in, IDS),
        load(weights_in, RW),
        load(mixed.at[:, mine], MP),
        load(cotangent.at[:, mine], CP),
    ]
    greet(n, t, s)
    for made in first_loads:
        made.wait()
    row_loads = [load(mixed, M), load(cotangent, C)]
    mix_loads = [
        load(decay_in, LD),
        load(writes_in, WK),
        load(values_in, TV),
        load(reads_in, RK),
        load(gate_in, OGT),
    ]
    expert_loads = [
        load(w_gate, W2.at[:, pl.ds(0, hid)]),
        load(w_up, W2.at[:, pl.ds(hid, hid)]),
        load(w_down, WD),
    ]
    proj_load = load(proj_in, OP)

    rows_n = max(n, 8)
    lane = lax.broadcasted_iota(jnp.int32, (rows_n, tok), 0) ^ s
    names = [IDS[i : i + 1, :] == lane for i in range(IDS.shape[0])]
    member = functools.reduce(jnp.logical_or, names)
    weight = sum(jnp.where(names[i], RW[i : i + 1, :], 0.0) for i in range(IDS.shape[0]))
    row_of = lax.broadcasted_iota(jnp.int32, (tok, tok), 0)
    col_of = lax.broadcasted_iota(jnp.int32, (tok, tok), 1)
    earlier = (row_of < col_of).astype(F32).astype(BF16)
    slot = dot(member.astype(F32).astype(BF16), earlier)
    slot = jnp.where(member, slot, -1.0).astype(jnp.int32)
    place = lax.broadcasted_iota(jnp.int32, (cap, tok), 0)

    z_slots = [[links.slot() for _ in range(n)] for _ in range(2)]
    m_part, c_part = MP[...], CP[...]
    for k in list(range(1, n)) + [0]:
        rows = pl.ds(k * cap, cap)
        chosen = slot[k : k + 1, :] == place
        pick = chosen.astype(F32).astype(BF16)
        row_weight = jnp.sum(jnp.where(chosen, weight[k : k + 1, :], 0.0), axis=1, keepdims=True)
        ONE[rows, :] = pick
        if k:
            SX[k - 1] = dot(pick, m_part).astype(BF16)
            SS[k - 1] = (dot(pick, c_part) * row_weight).astype(BF16)
            for a, (src, dst) in enumerate(((SX, X), (SS, S))):
                links.start(z_slots[a][k], src.at[k - 1], dst.at[rows, mine], {"sp": s ^ k})
        else:
            WCOL[...] = jnp.broadcast_to(row_weight, WCOL.shape)

    def local_rows():
        for made in row_loads:
            made.wait()

        def some(i, _):
            at = pl.ds(pl.multiple_of(i * share, 128), share)
            pick = ONE[pl.ds(0, cap), :]
            X[pl.ds(0, cap), at] = dot(pick, M[:, at]).astype(BF16)
            S[pl.ds(0, cap), at] = (dot(pick, C[:, at]) * WCOL[:, :1]).astype(BF16)
            return 0

        lax.fori_loop(0, ranks, some, 0)

    chunks = {}
    for q in range(blocks):
        first = cap if q == 0 else 0
        if first == R:
            continue
        for a, ref in enumerate((X, S)):

            def window(bits, part, ref=ref, row=q * R + first, count=R - first):
                begin, size = (t ^ bits) * share, share
                if part is not None:
                    begin, size = begin + part * half_share, half_share
                return ref.at[pl.ds(row, count), pl.ds(pl.multiple_of(begin, 128), size)]

            chunks[(q, a)] = Spread(links, t, window)

    def p0(q, a):
        ref = (X, S)[a]
        for k in range(q * group, (q + 1) * group):
            if k:
                links.arrived(z_slots[a][k], ref.at[pl.ds(k * cap, cap), mine], {"sp": s ^ k})
        chunks[(q, a)].p0()

    def expert_a(q):
        r = pl.ds(q * R, R)
        both = dot(X[r, :], W2[...])
        gate, up = both[:, :hid], both[:, hid:]
        sigma = jax.nn.sigmoid(gate)
        act = gate * sigma
        HID[r, :] = (act * up).astype(BF16)
        ACT[...] = act
        DFAC[...] = up * sigma * (1.0 + gate * (1.0 - sigma))

    def expert_b(q):
        r = pl.ds(q * R, R)
        d_act = dot(S[r, :], WD[...], 1, 1)
        DGU[r, pl.ds(0, hid)] = (d_act * DFAC[...]).astype(BF16)
        DGU[r, pl.ds(hid, hid)] = (d_act * ACT[...]).astype(BF16)

    def portion(q):
        r = pl.ds(q * R, R)
        step = 256
        for j in range(pieces):

            def some(i, _, j=j):
                begin = pl.multiple_of(j * strip + i * step, 128)
                tile = dot(DGU[r, :], W2[pl.ds(begin, step), :], 1, 1).astype(BF16)
                if pw >= step:
                    per = pw // step
                    dest, off = i // per, lax.rem(i, per) * step
                    at = pl.ds(pl.multiple_of(j * pw + off, 128), step)
                    PB[q, lax.rem(dest, 2), dest // 4, lax.rem(dest // 2, 2), :, at] = tile
                else:
                    at = pl.ds(j * pw, pw)
                    PB[q, 0, i // 2, lax.rem(i, 2), :, at] = tile[:, :pw]
                    PB[q, 1, i // 2, lax.rem(i, 2), :, at] = tile[:, pw:]
                return 0

            lax.fori_loop(0, strip // step, some, 0)

    rs_slots = [[links.slot() for _ in range(5)] for _ in range(blocks)]
    back_slots = [links.slot() for _ in range(n)]
    lo, hi = pl.ds(0, half_share), pl.ds(half_share, half_share)

    def r0(q):
        links.start(rs_slots[q][0], PB.at[q, 1 - c], RB.at[q], other)

    def r1(q):
        links.arrived(rs_slots[q][0], RB.at[q], other)

        def add(i, _):
            a, b = i // 2, lax.rem(i, 2)
            RB[q, a, b] = (PB[q, c, a, b].astype(F32) + RB[q, a, b].astype(F32)).astype(BF16)
            return 0

        lax.fori_loop(0, ranks // 2, add, 0)
        links.start(rs_slots[q][1], RB.at[q, :, 1 - mx, :, lo], RX.at[q], across)
        links.start(rs_slots[q][2], RB.at[q, 1 - my, :, :, hi], RY.at[q], along)

    def r2(q):
        links.arrived(rs_slots[q][1], RX.at[q], across)
        for i in range(2):
            RX[q, i] = (RB[q, i, mx, :, lo].astype(F32) + RX[q, i].astype(F32)).astype(BF16)
        links.start(rs_slots[q][3], RX.at[q, 1 - my], RX2.at[q], along)
        links.arrived(rs_slots[q][2], RY.at[q], along)
        for i in range(2):
            RY[q, i] = (RB[q, my, i, :, hi].astype(F32) + RY[q, i].astype(F32)).astype(BF16)
        links.start(rs_slots[q][4], RY.at[q, 1 - mx], RY2.at[q], across)

    def r3(q):
        r = pl.ds(q * R, R)
        links.arrived(rs_slots[q][3], RX2.at[q], along)
        FIN[r, lo] = (RX[q, my].astype(F32) + RX2[q].astype(F32)).astype(BF16)
        links.arrived(rs_slots[q][4], RY2.at[q], across)
        FIN[r, hi] = (RY[q, mx].astype(F32) + RY2[q].astype(F32)).astype(BF16)
        for k in range(q * group, (q + 1) * group):
            rows = pl.ds(k * cap, cap)
            if k:
                links.start(back_slots[k], FIN.at[rows, :], CB.at[rows, :], {"sp": s ^ k})
            else:
                CB[rows, :] = FIN[rows, :]

    def grads_gate_up(first, last):
        def some(i, _):
            at = pl.ds(pl.multiple_of(i * 256, 128), 256)
            tile = dot(X[:, at], DGU[...], 0, 0).astype(BF16)
            GW[at, :] = tile[:, :hid]
            UW[at, :] = tile[:, hid:]
            return 0

        lax.fori_loop(first, last, some, 0)

    def grads_down():
        HT[...] = HID[...].T

        def some(i, _):
            at = pl.ds(pl.multiple_of(i * 512, 128), 512)
            DW[:, at] = dot(HT[...], S[:, at]).astype(BF16)
            return 0

        lax.fori_loop(0, width // 512, some, 0)

    head_of = lax.broadcasted_iota(jnp.int32, (tok, chan), 1) // HEAD_DIM
    end_slots = [[links.slot() for _ in range(n)] for _ in range(2)]
    gated_slots = [links.slot() for _ in range(n)]
    state_slots = [links.slot() for _ in range(n)]

    def keys(ref, g):
        return ref[:, g * STATE : (g + 1) * STATE]

    def wide(columns):
        return jnp.concatenate(
            [jnp.broadcast_to(columns[:, h : h + 1], (tok, HEAD_DIM)) for h in range(heads)], axis=1
        )

    def everyone(slots, src, dst):
        for k in range(1, n):
            links.start(slots[k], src, dst(k), {"sp": s ^ k})

    def mixer_ends():
        for made in mix_loads:
            made.wait()
        pad = max(heads, 8) - heads
        decays = LD[...]
        if pad:
            decays = jnp.concatenate([decays, jnp.zeros((pad, tok), F32)], axis=0)
        upto = (row_of <= col_of).astype(F32)
        cumul = lax.dot_general(
            decays,
            upto,
            (((1,), (0,)), ((), ())),
            precision=lax.Precision.HIGHEST,
            preferred_element_type=F32,
        )
        total = cumul[:, tok - 1 :]
        TOT[s] = jnp.broadcast_to(total, TOT.shape[1:])
        columns = cumul.T
        spread = wide(columns)
        LW[...] = jnp.exp(spread)
        tails = jnp.exp(spread[tok - 1 :, :] - spread)
        TW[...] = tails
        TLD[...] = (TV[...].astype(F32) * tails).astype(BF16)
        for g in range(groups):
            at = pl.ds(g * chan, chan)
            END[s, at, :] = dot(TLD[:, at], keys(WK, g), 0, 0).astype(BF16)
        everyone(end_slots[0], END.at[s], lambda k: END.at[s])
        everyone(end_slots[1], TOT.at[s], lambda k: TOT.at[s])
        for h in range(heads):
            span = columns[:, h : h + 1] - cumul[h : h + 1, :]
            DEC[h] = jnp.exp(jnp.where(row_of >= col_of, span, -jnp.inf))

    def mixer_inner():
        for g in range(groups):
            scores = dot(keys(RK, g), keys(WK, g), 1, 1)
            at = pl.ds(g * chan, chan)
            inner = jnp.zeros((tok, chan), F32)
            for r in range(per_group):
                h = g * per_group + r
                kept = scores * DEC[h]
                KT[h] = kept.T.astype(BF16)
                inner = jnp.where(head_of == r, dot(kept.astype(BF16), TV[:, at]), inner)
            Y[:, at] = inner

    def factor(j):
        return jnp.concatenate(
            [jnp.broadcast_to(jnp.exp(TOT[j][h : h + 1, :]), (HEAD_DIM, STATE)) for h in range(heads)],
            axis=0,
        )

    def mixer_gated():
        for k in range(1, n):
            links.arrived(end_slots[0][k], END.at[s ^ k], {"sp": s ^ k})
            links.arrived(end_slots[1][k], TOT.at[s ^ k], {"sp": s ^ k})
        state = jnp.zeros(END.shape[1:], F32)
        for j in range(n - 1):
            state = jnp.where(j < s, factor(j) * state + END[j].astype(F32), state)
        ENT[...] = state.astype(BF16)
        for g in range(groups):
            at = pl.ds(g * chan, chan)
            carried = dot(keys(RK, g), ENT[at, :], 1, 1)
            y = Y[:, at] + carried * LW[:, at]
            Y[:, at] = y
            gate = OGT[:, at].astype(F32)
            GB[pl.ds(0, tok), at] = (y * (gate * jax.nn.sigmoid(gate))).astype(BF16)
        if pieces == n:
            own = GB.at[pl.ds(0, tok), :]
            everyone(gated_slots, own, lambda k: GB.at[pl.ds(k * tok, tok), :])

    def mixer_states():
        for g in range(groups):
            at = pl.ds(g * chan, chan)
            gate = OGT[:, at].astype(F32)
            sig = jax.nn.sigmoid(gate)
            outer = OG[:, at] * (gate * sig)
            OB[:, at] = outer.astype(BF16)
            LED[:, at] = (outer * LW[:, at]).astype(BF16)
            BK[s, at, :] = dot(LED[:, at], keys(RK, g), 0, 0).astype(BF16)
        everyone(state_slots, BK.at[s], lambda k: BK.at[s])

    def mixer_scores():
        for g in range(groups):
            at = pl.ds(g * chan, chan)
            gate = OGT[:, at].astype(F32)
            sig = jax.nn.sigmoid(gate)
            DGT[:, at] = (OG[:, at] * Y[:, at] * sig * (1.0 + gate * (1.0 - sig))).astype(BF16)
            d_scores = jnp.zeros((tok, tok), F32)
            d_values = jnp.zeros((tok, chan), F32)
            for r in range(per_group):
                h = g * per_group + r
                one = jnp.where(head_of == r, OB[:, at].astype(F32), 0.0).astype(BF16)
                d_scores = d_scores + dot(one, TV[:, at], 1, 1) * DEC[h]
                d_values = jnp.where(head_of == r, dot(KT[h], OB[:, at]), d_values)
            OG[:, at] = d_values
            d_scores = d_scores.astype(BF16)
            ks = pl.ds(g * STATE, STATE)
            DRK[:, ks] = (dot(d_scores, keys(WK, g)) + dot(LED[:, at], ENT[at, :])).astype(BF16)
            DWF[:, ks] = dot(d_scores, keys(RK, g), 0, 0)

    def mixer_last():
        for k in range(1, n):
            links.arrived(state_slots[k], BK.at[s ^ k], {"sp": s ^ k})
        state = jnp.zeros(BK.shape[1:], F32)
        for j in range(n - 1, 0, -1):
            state = jnp.where(j > s, factor(j) * state + BK[j].astype(F32), state)
        leaving = state.astype(BF16)
        for g in range(groups):
            at = pl.ds(g * chan, chan)
            ks = pl.ds(g * STATE, STATE)
            mine_of = leaving[g * chan : (g + 1) * chan]
            DWK[:, ks] = (DWF[:, ks] + dot(TLD[:, at], mine_of)).astype(BF16)
            d_values = OG[:, at] + dot(keys(WK, g), mine_of, 1, 1) * TW[:, at]
            DV[:, at] = d_values.astype(BF16)

    order = [key for key in chunks]
    count = len(order)

    def forward(i):
        if i < count:
            p0(*order[i])
        if 0 <= i - 1 < count:
            chunks[order[i - 1]].p1()
        if 0 <= i - 2 < count:
            chunks[order[i - 2]].p2()

    def landed(q, a):
        if (q, a) in chunks:
            chunks[(q, a)].p3()

    def rest(q):
        landed(q, 1)
        expert_b(q)
        portion(q)
        r0(q)

    def add_back(first, last, start):
        rows = pl.ds(first * cap, (last - first) * cap)
        for k in range(max(first, 1), last):
            one = pl.ds(k * cap, cap)
            links.arrived(back_slots[k], CB.at[one, :], {"sp": s ^ k})
        part = dot(ONE[rows, :], CB[rows, :], 0, 0)
        BACK[...] = part if start else BACK[...] + part

    tiles = width // 256
    mixer_ends()
    if blocks == 4 and (0, 0) not in chunks:
        forward(0)
        local_rows()
        for made in expert_loads:
            made.wait()
        forward(1)
        expert_a(0)
        expert_b(0)
        forward(2)
        portion(0)
        r0(0)
        forward(3)
        mixer_inner()
        landed(1, 0)
        expert_a(1)
        forward(4)
        rest(1)
        forward(5)
        r1(1)
        mixer_gated()
        landed(2, 0)
        expert_a(2)
        forward(6)
        rest(2)
        forward(7)
        r2(1)
        r1(2)
        landed(3, 0)
        expert_a(3)
        rest(3)
        r3(1)
        r2(2)
        r1(3)
        r1(0)
        grads_gate_up(0, tiles // 8)
        r3(2)
        r2(3)
        grads_gate_up(tiles // 8, tiles // 4)
        r2(0)
        r3(3)
        grads_gate_up(tiles // 4, tiles)
        add_back(1, 3, True)
        r3(0)
        add_back(0, 1, False)
        add_back(3, 4, False)
    else:
        local_rows()
        for made in expert_loads:
            made.wait()
        mixer_inner()
        mixer_gated()
        for i in range(count + 2):
            forward(i)
        for q in range(blocks):
            landed(q, 0)
            expert_a(q)
            rest(q)
        for stage in (r1, r2, r3):
            for q in range(blocks):
                stage(q)
        grads_gate_up(0, tiles // 2)
        add_back(0, n, True)

    half_tok = tok // 2
    cuts = 2
    cut = tok // cuts
    gathers = []
    for i in range(cuts):

        def window(bits, part, i=i):
            row, rows = i * cut, cut
            if part is not None:
                row, rows = row + part * (cut // 2), cut // 2
            return G.at[:, pl.ds(row, rows), pl.ds(pl.multiple_of((t ^ bits) * pw, 128), pw)]

        gathers.append(Spread(links, t, window))
    here = pl.ds(pl.multiple_of(t * pw, 128), pw)
    for i in range(cuts):
        rows = pl.ds(i * cut, cut)
        for j in range(pieces):
            cot = C[rows, pl.ds(pl.multiple_of(j * strip + t * pw, 128), pw)].astype(F32)
            G[j, rows, here] = (cot + BACK[rows, pl.ds(j * pw, pw)]).astype(BF16)
        gathers[i].p0()

    fars = []
    if pieces == n:
        far_slots = [links.slot() for _ in range(n)]
        for k in range(1, n):
            rows = pl.ds((k - 1) * tok, tok)
            links.start(far_slots[k], G.at[s ^ k, :, here], F.at[rows, here], {"sp": s ^ k})

            def window(bits, part, k=k):
                row, rows = (k - 1) * tok, tok
                if part is not None:
                    row, rows = row + part * half_tok, half_tok
                return F.at[pl.ds(row, rows), pl.ds(pl.multiple_of((t ^ bits) * pw, 128), pw)]

            fars.append(Spread(links, t, window))

    def far_p0(k):
        rows = pl.ds((k - 1) * tok, tok)
        links.arrived(far_slots[k], F.at[rows, here], {"sp": s ^ k})
        fars[k - 1].p0()

    grads_down()
    for i in range(cuts):
        gathers[i].p1()
        if i:
            gathers[i - 1].p2()
    gathers[cuts - 1].p2()
    for k in range(1, len(fars) + 1):
        far_p0(k)
    for i in range(cuts):
        gathers[i].p3()
    proj_load.wait()
    OG[...] = sum(dot(G[j], OP[pl.ds(j * strip, strip), :]) for j in range(pieces))
    def proj_own(i, _):
        at = pl.ds(pl.multiple_of(i * 256, 128), 256)
        PJ[at, :] = dot(G[s, :, at], GB[pl.ds(0, tok), :], 0, 0)
        return 0

    def proj_far(i, _):
        at = pl.ds(pl.multiple_of(i * 256, 128), 256)
        PJ[at, :] += dot(F[:, at], GB[pl.ds(tok, (n - 1) * tok), :], 0, 0)
        return 0

    mixer_states()
    for far in fars:
        far.p1()
    mixer_scores()
    for far in fars:
        far.p2()
    if pieces == n:
        lax.fori_loop(0, strip // 256, proj_own, 0)
    mixer_last()
    if pieces == n:
        for far in fars:
            far.p3()
        for k in range(1, n):
            links.arrived(gated_slots[k], GB.at[pl.ds(k * tok, tok), :], {"sp": s ^ k})
        lax.fori_loop(0, strip // 256, proj_far, 0)
    else:
        for j in range(pieces):
            outs_proj[0][:, pl.ds(j * strip, strip)] = G[j]
        outs_proj[1][...] = GB[pl.ds(0, tok), :]
    links.finish()


def place_kernel(count, *refs):
    sources, places, sem = refs[:count], refs[count : 2 * count], refs[-1]
    made = [pltpu.make_async_copy(sources[i], places[i], sem.at[i]) for i in range(count)]
    for one in made:
        one.start()
    for one in made:
        one.wait()


def place(arrays):
    any_ = pl.BlockSpec(memory_space=pl.ANY)
    count = len(arrays)
    return pl.pallas_call(
        functools.partial(place_kernel, count),
        out_shape=[jax.ShapeDtypeStruct(a.shape, a.dtype) for a in arrays],
        in_specs=[any_] * count,
        out_specs=[any_] * count,
        scratch_shapes=[pltpu.SemaphoreType.DMA((count,))],
        compiler_params=pltpu.CompilerParams(vmem_limit_bytes=1024 * 1024),
    )(*arrays)


def body(
    token_values,
    write_keys,
    read_keys,
    log_decay,
    out_gate,
    out_proj,
    mixed,
    cotangent,
    route_ids,
    route_weights,
    w_gate,
    w_up,
    w_down,
):
    tok, width = mixed.shape
    n = lax.axis_size("sp")
    ranks = lax.axis_size("tp")
    hid = w_gate.shape[2]
    inner = token_values.shape[1]
    heads = log_decay.shape[0]
    share = width // ranks
    cap = 3 * tok // n
    rows = n * cap
    pieces = n if (width // n // ranks) % 128 == 0 else 1
    far = pieces == n
    strip = width // pieces
    blocks = 4 if n % 4 == 0 else n
    R = rows // blocks
    slots = 2 * n + 2 * blocks * 9 + 5 * blocks + 6 * n + 18 + 9 * n
    any_ = pl.BlockSpec(memory_space=pl.ANY)

    def buf(*shape, dtype=BF16):
        return pltpu.VMEM(shape, dtype)

    def like(a):
        return pltpu.VMEM(a.shape, a.dtype)

    if far:
        proj_shapes = [pltpu.VMEM((strip, inner), F32)]
    else:
        proj_shapes = [pltpu.VMEM((tok, width), BF16), pltpu.VMEM((tok, inner), BF16)]
    operands = [
        route_ids.T,
        route_weights.T,
        mixed,
        cotangent,
        w_gate[0],
        w_up[0],
        w_down[0],
        token_values,
        write_keys,
        read_keys,
        log_decay,
        out_gate,
        out_proj,
    ]
    outputs = (
        [like(token_values), like(write_keys), like(read_keys), like(out_gate)]
        + [like(w_gate[0]), like(w_up[0]), like(w_down[0])]
        + proj_shapes
    )
    got = pl.pallas_call(
        functools.partial(main_kernel, n, ranks, pieces),
        out_shape=outputs,
        in_specs=[any_] * len(operands),
        out_specs=[pl.BlockSpec(memory_space=pltpu.VMEM)] * len(outputs),
        scratch_shapes=[
            buf(*route_ids.T.shape, dtype=jnp.int32),
            buf(*route_ids.T.shape, dtype=F32),
            buf(tok, width),
            buf(tok, width),
            buf(width, 2 * hid),
            buf(hid, width),
            buf(rows, width),
            buf(rows, width),
            buf(n - 1, cap, share),
            buf(n - 1, cap, share),
            buf(rows, tok),
            buf(cap, 128, dtype=F32),
            buf(rows, 2 * hid),
            buf(rows, hid),
            buf(hid, rows),
            buf(blocks, 2, 2, ranks // 4, R, share),
            buf(blocks, 2, ranks // 4, R, share),
            buf(blocks, 2, R, share // 2),
            buf(blocks, 2, R, share // 2),
            buf(blocks, R, share // 2),
            buf(blocks, R, share // 2),
            buf(rows, share),
            buf(rows, share),
            buf(pieces, tok, strip),
            buf(*token_values.shape),
            buf(*write_keys.shape),
            buf(*read_keys.shape),
            buf(*log_decay.shape, dtype=F32),
            buf(*out_gate.shape),
            buf(*out_proj.shape),
            buf(tok, inner, dtype=F32),
            buf(tok, inner, dtype=F32),
            buf(tok, inner, dtype=F32),
            buf(heads, tok, tok, dtype=F32),
            buf(heads, tok, tok),
            buf(tok, inner),
            buf(n, inner, STATE),
            buf(n, max(heads, 8), STATE, dtype=F32),
            buf(n, inner, STATE),
            buf(inner, STATE),
            buf(n * tok if far else tok, inner),
            buf((n - 1) * tok if far else 16, strip if far else 128),
            buf(tok, inner, dtype=F32),
            buf(tok, inner),
            buf(tok, inner),
            buf(*write_keys.shape, dtype=F32),
            buf(tok, share),
            buf(tok, share),
            buf(R, hid, dtype=F32),
            buf(R, hid, dtype=F32),
            buf(tok, share, dtype=F32),
            pltpu.SemaphoreType.DMA((slots,)),
            pltpu.SemaphoreType.DMA((slots,)),
            pltpu.SemaphoreType.DMA((24 + pieces,)),
        ],
        compiler_params=pltpu.CompilerParams(
            collective_id=1, has_side_effects=True, vmem_limit_bytes=VMEM_LIMIT
        ),
    )(*operands)
    placed = place(got if far else got[:7])
    value_grad, write_grad, read_grad, gate_grad, grad_gate, grad_up, grad_down = placed[:7]
    if far:
        proj_grad = placed[7]
    else:
        proj_part = dot(got[7], got[8], 0, 0).astype(BF16)
        proj_grad = lax.psum_scatter(proj_part, "sp", scatter_dimension=0, tiled=True).astype(F32)
    return (
        value_grad,
        write_grad,
        read_grad,
        gate_grad,
        proj_grad,
        grad_gate[None],
        grad_up[None],
        grad_down[None],
    )


def solution(mesh):
    return jax.shard_map(
        body,
        mesh=mesh,
        in_specs=(
            P("sp", "tp"),
            P("sp", "tp"),
            P("sp", "tp"),
            P("tp", "sp"),
            P("sp", "tp"),
            P(None, "tp"),
            P("sp", None),
            P("sp", None),
            P("sp", None),
            P("sp", None),
            P("sp", None, "tp"),
            P("sp", None, "tp"),
            P("sp", "tp", None),
        ),
        out_specs=(
            P("sp", "tp"),
            P("sp", "tp"),
            P("sp", "tp"),
            P("sp", "tp"),
            P("sp", "tp"),
            P("sp", None, "tp"),
            P("sp", None, "tp"),
            P("sp", "tp", None),
        ),
        check_vma=False,
    )
```
